32 devices in a mesh: sp: 8 (over z, y), tp: 4 (over x, core).
Axes of the slice: x: 2, y: 2, z: 4, core: 2. Of those that a mesh axis runs over, the one named last changes fastest.
Arguments:
- stream: bfloat16 [4096, 2048], P('sp', 'tp'), may hold values from -6 to 6
- doc_ids: int32 [4096], P('sp'), may hold values from 0 to 3, never falling along the last dimension, each value on 1 to 2304 neighbouring positions
- norm_gain: float32 [2, 2048], replicated, may hold values from 0.1 to 1.9
- gate_proj: bfloat16 [2, 2048, 2048], P(None, 'sp', 'tp'), may hold values from -0.125 to 0.125
- input_gate: bfloat16 [2, 2048, 2048], P(None, 'sp', 'tp'), may hold values from -0.125 to 0.125
- value_proj: bfloat16 [2, 2048, 2048], P(None, 'sp', 'tp'), may hold values from -0.125 to 0.125
- taps: float32 [2, 3, 2048], P(None, None, 'tp'), may hold values from -3 to 3
- out_proj: bfloat16 [2, 2048, 2048], P(None, 'tp', 'sp'), may hold values from -0.125 to 0.125
Outputs:
- result: bfloat16 [4096, 2048], P('sp', 'tp')
The draws below stay inside these ranges and needn't reach their ends.
Inputs may be any that keep to these rules, and one draw needn't show every extreme that they name: `doc_ids`: document numbers never fall along the sequence; each document holds 1 to 2304 positions.
All inputs are finite; a program needn't handle non-finite values.
Results may differ from the reference program's by a relative error of at most 0.03.
Values may be sent and summed in bfloat16 or wider, within the bound.
A program may use at most 64 MiB of HBM per device.

```python
import math
import jax
import jax.numpy as jnp
import numpy as np
from jax import lax

D = 2048
CW = 2048
LAYERS = 2
TOKENS = 4096
DOCS = 4
DOC_MOST = 2304
N_TP = 4


def steps_of(rng, dims, cuts, least, high):
    def one(dim, blocks):
        draws = jax.random.uniform(jax.random.fold_in(jax.random.fold_in(rng, 6), dim), (blocks,), jnp.float32, least / len(cuts), high / len(cuts))
        return jnp.repeat(jnp.exp(draws), dims[dim] // blocks).reshape((-1,) + (1,) * (len(dims) - dim - 1))

    loudness = one(*cuts[0])
    for cut in cuts[1:]:
        loudness = loudness * one(*cut)
    return loudness


def length_profile(amount, total, bound, lean):
    loads = [(1 << 20) // math.isqrt(grade ** lean) + 1 for grade in range(2, amount + 1)]
    surplus, holding = total - bound - (amount - 1), [1] * (amount - 1)
    while surplus > 0:
        candidates = [i for i in range(amount - 1) if holding[i] < bound]
        pool, left = sum([loads[i] for i in candidates]), surplus
        for i in candidates:
            addition = min(bound - holding[i], max(1, left * loads[i] // pool), surplus)
            holding[i] = holding[i] + addition
            surplus = surplus - addition
    return np.array([bound] + holding)


def ragged_sizes(own_key, amount, total, most, slope):
    if amount == 2:
        one = jax.random.randint(own_key, (), max(1, total - most), min(most, total - 1) + 1)
        return jnp.stack([one, total - one])
    sizes = jnp.asarray(length_profile(amount, total, most, slope), jnp.int32)
    pairs = (amount - 1) // 2
    source_of, taker = sizes[1:1 + 2 * pairs:2], sizes[2:2 + 2 * pairs:2]
    room = jnp.minimum(source_of - 1, most - taker)
    moved = jax.random.randint(jax.random.fold_in(own_key, 1), (pairs,), 0, 1 << 20) % (room + 1)
    sizes = sizes.at[1:1 + 2 * pairs:2].set(source_of - moved).at[2:2 + 2 * pairs:2].set(taker + moved)
    return sizes[jax.random.permutation(jax.random.fold_in(own_key, 2), amount)]


def noise(stream_key, shape, spread, limit, split=(), kind=jnp.bfloat16):
    entries = spread * jax.random.normal(stream_key, shape, jnp.float32)
    if split:
        entries = entries * steps_of(stream_key, shape, split, -0.22, 0.18)
    return jnp.clip(entries, -limit, limit).astype(kind)


def setup_inputs(seed: int = 0) -> dict:
    key_of = jax.random.split(jax.random.key(seed), 9)
    return {
        "stream": noise(key_of[0], (TOKENS, D), 1.0, 6.0, ((0, 8), (1, 4))),
        "doc_ids": jnp.searchsorted(jnp.cumsum(ragged_sizes(key_of[1], DOCS, TOKENS, DOC_MOST, 1)), jnp.arange(TOKENS), side="right").astype(jnp.int32),
        "norm_gain": jnp.clip(1.0 + 0.18 * jax.random.normal(key_of[2], (LAYERS, D), jnp.float32), 0.1, 1.9),
        "gate_proj": noise(key_of[3], (LAYERS, D, CW), D ** -0.5, 0.125, ((1, 8), (2, 4))),
        "input_gate": noise(key_of[4], (LAYERS, D, CW), D ** -0.5, 0.125, ((1, 8), (2, 4))),
        "value_proj": noise(key_of[5], (LAYERS, D, CW), D ** -0.5, 0.125, ((1, 8), (2, 4))),
        "taps": noise(key_of[6], (LAYERS, 3, CW), 0.5, 3.0, ((2, 4),), jnp.float32),
        "out_proj": noise(key_of[7], (LAYERS, CW, D), CW ** -0.5, 0.125, ((1, 4), (2, 8))),
    }


epsilon = 1e-06

def reference(stream, doc_ids, norm_gain, gate_proj, input_gate, value_proj, taps, out_proj):
    block = CW // N_TP
    current = stream
    for layer_index in range(LAYERS):
        widened = current.astype(jnp.float32)
        scale = lax.rsqrt(lax.optimization_barrier(jnp.mean(widened * widened, axis=-1, keepdims=True)) + epsilon)
        normed = (widened * scale * norm_gain[layer_index]).astype(jnp.bfloat16)
        gate_b = jnp.dot(normed, gate_proj[layer_index], preferred_element_type=jnp.float32).astype(jnp.bfloat16)
        gate_c = jnp.dot(normed, input_gate[layer_index], preferred_element_type=jnp.float32).astype(jnp.bfloat16)
        values = jnp.dot(normed, value_proj[layer_index], preferred_element_type=jnp.float32).astype(jnp.bfloat16)
        mixed_in = (gate_c.astype(jnp.float32) * values.astype(jnp.float32)).astype(jnp.bfloat16)
        mixed_wide = mixed_in.astype(jnp.float32)
        zero_row = jnp.zeros((1, CW), jnp.float32)
        before = jnp.concatenate([zero_row, mixed_wide[:-1]], axis=0)
        after = jnp.concatenate([mixed_wide[1:], zero_row], axis=0)
        same_doc = doc_ids[1:] == doc_ids[:-1]
        false_edge = jnp.zeros((1,), bool)
        same_prev = jnp.concatenate([false_edge, same_doc])[:, None]
        same_next = jnp.concatenate([same_doc, false_edge])[:, None]
        kernel_taps = taps[layer_index]
        convolved = jnp.where(same_prev, kernel_taps[0] * before, 0.0) + kernel_taps[1] * mixed_wide + jnp.where(same_next, kernel_taps[2] * after, 0.0)
        gated = (gate_b.astype(jnp.float32) * convolved).astype(jnp.bfloat16)
        total = jnp.zeros((TOKENS, D), jnp.float32)
        for block_index in range(N_TP):
            lower = block_index * block
            partial_value = jnp.dot(gated[:, lower:lower + block], out_proj[layer_index][lower:lower + block], preferred_element_type=jnp.float32).astype(jnp.bfloat16)
            total = total + partial_value.astype(jnp.float32)
        current = (current.astype(jnp.float32) + total).astype(jnp.bfloat16)
    return current
```

```python
import functools

import jax
import jax.numpy as jnp
from jax import lax
from jax.experimental import pallas as pl
from jax.experimental.pallas import tpu as pltpu
from jax.sharding import PartitionSpec as P

epsilon = 1e-06


def with_halo(value, sides, width):
    for axis, dim in sides:
        size, length = (lax.axis_size(axis), value.shape[dim])
        up = [(i, (i + 1) % size) for i in range(size - 1)]
        down = [(j, i) for i, j in up]
        last = lax.slice_in_dim(value, length - width, length, axis=dim)
        leading = lax.slice_in_dim(value, 0, width, axis=dim)
        before = lax.ppermute(last, axis, up)
        after = lax.ppermute(leading, axis, down)
        value = jnp.concatenate([before, value, after], axis=dim)
    return value


def per_device(stream, doc_ids, norm_gain, gate_proj, input_gate, value_proj, taps, out_proj):
    layers = gate_proj.shape[0]
    gathered_in = (
        lax.all_gather(gate_proj, "sp", axis=1, tiled=True),
        lax.all_gather(input_gate, "sp", axis=1, tiled=True),
        lax.all_gather(value_proj, "sp", axis=1, tiled=True),
    )
    gathered_out = lax.all_gather(out_proj, "sp", axis=2, tiled=True)
    current = stream
    for layer_index in range(layers):
        full_rows = lax.all_gather(current, "tp", axis=1, tiled=True)
        widened = full_rows.astype(jnp.float32)
        scale = lax.rsqrt(jnp.mean(widened * widened, axis=-1, keepdims=True) + epsilon)
        normed = (widened * scale * norm_gain[layer_index]).astype(jnp.bfloat16)
        gate_b = jnp.dot(normed, gathered_in[0][layer_index], preferred_element_type=jnp.float32)
        gate_c = jnp.dot(normed, gathered_in[1][layer_index], preferred_element_type=jnp.float32)
        values = jnp.dot(normed, gathered_in[2][layer_index], preferred_element_type=jnp.float32)
        gate_b = gate_b.astype(jnp.bfloat16)
        gate_c = gate_c.astype(jnp.bfloat16)
        values = values.astype(jnp.bfloat16)
        mixed_in = (gate_c.astype(jnp.float32) * values.astype(jnp.float32)).astype(jnp.bfloat16)
        padded, doc_padded = (
            with_halo(mixed_in, (("sp", 0),), 1),
            with_halo(doc_ids, (("sp", 0),), 1),
        )
        same_prev = (doc_padded[:-2] == doc_ids)[:, None]
        same_next = (doc_padded[2:] == doc_ids)[:, None]
        kernel_taps = taps[layer_index]
        convolved = (
            jnp.where(same_prev, kernel_taps[0] * padded[:-2].astype(jnp.float32), 0.0)
            + kernel_taps[1] * mixed_in.astype(jnp.float32)
            + jnp.where(same_next, kernel_taps[2] * padded[2:].astype(jnp.float32), 0.0)
        )
        gated = (gate_b.astype(jnp.float32) * convolved).astype(jnp.bfloat16)
        partials = jnp.dot(gated, gathered_out[layer_index], preferred_element_type=jnp.float32)
        summed = lax.psum_scatter(
            partials.astype(jnp.bfloat16), "tp", scatter_dimension=1, tiled=True
        ).astype(jnp.float32)
        current = (current.astype(jnp.float32) + summed).astype(jnp.bfloat16)
    return current


MESH = pl.DeviceIdType.MESH


def fused_kernel(S, T, L, stream_ref, docs_ref, gain_ref, gate_ref, input_ref, value_ref, taps_ref, outw_ref,
                 result_ref, win, wout, stage_in, stage_out, xfull, normed, cbuf, mpad, edge, halo, docall, docpad,
                 mprev, mnext, gated, dsrc, drcv, xsrc, xrcv, zsrc, zrcv, acc,
                 own_sem, w_send, y_send, w_recv, x_sem, agz_send, agx_send, agc_send, ag_recv,
                 d_send, d_recv, x_send, x_recv, z_send, z_recv, h_send, h_recv, doc_send, doc_recv):
    s = lax.axis_index("sp")
    t = lax.axis_index("tp")
    Z = S // 2
    z, y = s // 2, s % 2
    zh, zl = z // 2, z % 2
    x, c = t // 2, t % 2
    X = T // 2
    rows = stream_ref.shape[0]
    depth = gate_ref.shape[1]
    half = taps_ref.shape[2] // 2
    ow = outw_ref.shape[2]
    width = stream_ref.shape[1]
    per = width // ow
    units = 4 * L
    other_y = s + 1 - 2 * y
    sibling = t + 1 - 2 * c
    across = lax.rem(t + 2, T)
    mate = s + 2 - 4 * zl
    theirs = 1 - zl
    sources = (input_ref, value_ref, gate_ref)
    bf, f32 = jnp.bfloat16, jnp.float32
    pending = []

    barrier = pltpu.get_barrier_semaphore()

    def greet(sp_index, tp_index):
        pl.semaphore_signal(barrier, inc=1, device_id=(sp_index, tp_index), device_id_type=MESH)

    for k in range(1, S):
        greet(lax.rem(s + k, S), t)
    greet(s, sibling)
    greet(s, across)

    def remote(src, dst, send_sem, recv_sem, target):
        return pltpu.make_async_remote_copy(src_ref=src, dst_ref=dst, send_sem=send_sem, recv_sem=recv_sem,
                                            device_id=target, device_id_type=MESH)

    def go(copy_of):
        copy_of().start()
        pending.append(copy_of)

    def slot(u, shard):
        layer, part = u // 4, u % 4
        if part < 3:
            return win.at[layer * 3 + part, pl.ds(pl.multiple_of(shard * depth, depth), depth)]
        return wout.at[layer, shard]

    def stage(u):
        layer, part = u // 4, u % 4
        return stage_in.at[layer * 3 + part] if part < 3 else stage_out.at[layer]

    def own_copy(u, which):
        layer, part = u // 4, u % 4
        pick = pl.ds(pl.multiple_of((zl if which == 0 else theirs) * half, half), half)
        source = outw_ref.at[layer, pick, :] if part == 3 else sources[part].at[layer, :, pick]
        return pltpu.make_async_copy(source, slot(u, s) if which == 0 else stage(u), own_sem.at[u, which])

    def piece(layer, plane, owner, i):
        return xfull.at[layer, plane, owner, i]

    def x_copy(i):
        return pltpu.make_async_copy(stream_ref.at[:, i * ow:(i + 1) * ow], piece(0, zl, t, i), x_sem.at[i])

    for i in range(per):
        x_copy(i).start()
    for u in range(units):
        for which in range(2):
            own_copy(u, which).start()

    pl.semaphore_wait(barrier, S + 1)

    def z_copy(u, k):
        plane = lax.rem(z + k, Z)
        return remote(slot(u, s) if k % 2 == 0 else stage(u), slot(u, s), w_send.at[u, k], w_recv.at[u, s],
                      (2 * plane + y, t))

    def y_copy(u, plane):
        shard = 2 * plane + y
        return remote(slot(u, shard), slot(u, shard), y_send.at[u, plane], w_recv.at[u, shard], (other_y, t))

    def begin(u):
        if u >= units:
            return
        for which in range(2):
            own_copy(u, which).wait()
        for k in range(1, Z):
            go(lambda k=k: z_copy(u, k))
        go(lambda: y_copy(u, z))

    def arrived(u, shard):
        remote(slot(u, shard), slot(u, shard), y_send.at[u, z], w_recv.at[u, shard], (other_y, t)).wait_recv()

    def pump(u):
        if u >= units:
            return
        for k in range(1, Z):
            plane = lax.rem(z + k, Z)
            arrived(u, 2 * plane + y)
            go(lambda plane=plane: y_copy(u, plane))
        begin(u + 2)

    def need(u):
        for k in range(Z):
            plane = lax.rem(z + k, Z)
            arrived(u, 2 * plane + 1 - y)

    def agz(layer, i):
        return remote(piece(layer, zl, t, i), piece(layer, zl, t, i), agz_send.at[layer, i],
                      ag_recv.at[layer, zl, t, i], (mate, t))

    def agx(layer, plane, i):
        return remote(piece(layer, plane, t, i), piece(layer, plane, t, i), agx_send.at[layer, plane, i],
                      ag_recv.at[layer, plane, t, i], (s, across))

    def agc(layer, plane, owner, i):
        return remote(piece(layer, plane, owner, i), piece(layer, plane, owner, i),
                      agc_send.at[layer, plane, owner, i], ag_recv.at[layer, plane, owner, i], (s, sibling))

    def ag_wait(layer, plane, owner, i):
        remote(piece(layer, plane, owner, i), piece(layer, plane, owner, i), agz_send.at[layer, i],
               ag_recv.at[layer, plane, owner, i], (mate, t)).wait_recv()

    def ag_own(layer, i):
        go(lambda: agz(layer, i))
        go(lambda: agx(layer, zl, i))
        go(lambda: agc(layer, zl, t, i))

    def ag_from_z(layer, i):
        ag_wait(layer, theirs, t, i)
        go(lambda: agx(layer, theirs, i))
        go(lambda: agc(layer, theirs, t, i))

    def ag_from_x(layer, plane, i):
        ag_wait(layer, plane, across, i)
        go(lambda: agc(layer, plane, across, i))

    def ag_from_core(layer, plane):
        for i in range(per):
            ag_wait(layer, plane, sibling, i)
            ag_wait(layer, plane, lax.rem(sibling + 2, T), i)

    def doc_copy(k):
        return remote(docs_ref, docall.at[s], doc_send.at[k], doc_recv.at[s], (lax.rem(s + k, S), t))

    def group_block(b):
        return 2 * (2 * zh + b) + y

    def halo_copy(layer, b, side):
        target = lax.rem(group_block(b) + (1 if side == 0 else S - 1), S)
        core = 2 * (2 * (target // 4) + zl) + target % 2
        return remote(edge.at[layer, b, 1 - side], halo.at[layer, (target // 2) % 2, side],
                      h_send.at[layer, b, side], h_recv.at[layer, (target // 2) % 2, side], (core, t))

    def halo_wait(layer, b, side):
        remote(edge.at[layer, b, side], halo.at[layer, b, side], h_send.at[layer, b, side],
               h_recv.at[layer, b, side], (other_y, t)).wait_recv()

    for i in range(per):
        x_copy(i).wait()
        ag_own(0, i)
    for k in range(1, S):
        go(lambda k=k: doc_copy(k))
    begin(0)
    begin(1)

    small = rows // 8

    def norm(layer, plane):
        def step(r, carry):
            at = pl.ds(pl.multiple_of(r * small, small), small)
            total = jnp.zeros((small, 1), f32)
            for q in range(T):
                for i in range(per):
                    wide = xfull[layer, plane, q, i, at, :].astype(f32)
                    total = total + jnp.sum(wide * wide, axis=-1, keepdims=True)
            scale = lax.rsqrt(total / (width * T) + epsilon)
            for q in range(T):
                for i in range(per):
                    wide = xfull[layer, plane, q, i, at, :].astype(f32)
                    low = q * width + i * ow
                    gain = gain_ref[layer:layer + 1, low:low + ow]
                    normed[plane, at, low:low + ow] = (wide * scale * gain).astype(bf)
            return carry

        lax.fori_loop(0, rows // small, step, 0)

    def project(layer, part, plane):
        product = jnp.dot(normed[plane], win[layer * 3 + part], preferred_element_type=f32)
        return product.astype(bf)

    def both(layer, part, use):
        def step(e, carry):
            plane = lax.rem(zl + e, 2)
            use(plane, project(layer, part, plane))
            return carry

        lax.fori_loop(0, 2, step, 0)

    def keep_gate(plane, value):
        cbuf[plane] = value

    def mix(plane, value):
        mixed = (cbuf[plane].astype(f32) * value.astype(f32)).astype(bf)
        mpad[plane, 8:8 + rows, :] = mixed.astype(f32)

    def columns(block, row):
        line = docall[block, row:row + 1, :].astype(f32)
        return jnp.transpose(jnp.broadcast_to(line, (128, 128)))

    def masks():
        docall[s] = docs_ref[...]
        for k in range(1, S):
            remote(docs_ref, docall.at[lax.rem(s + k, S)], doc_send.at[k], doc_recv.at[lax.rem(s + k, S)],
                   (other_y, t)).wait_recv()
        lines = rows // 128
        for b in range(2):
            block = group_block(b)
            for j in range(lines):
                docpad[8 + 128 * j:136 + 128 * j, :] = columns(block, j)
            before = columns(lax.rem(block + S - 1, S), lines - 1)[120:128, :]
            after = columns(lax.rem(block + 1, S), 0)[0:8, :]
            docpad[0:8, :] = jnp.where(block > 0, before, -1.0)
            docpad[8 + rows:16 + rows, :] = jnp.where(block < S - 1, after, -1.0)
            here = docpad[8:8 + rows, :]
            mprev[b] = jnp.where(docpad[7:7 + rows, :] == here, 1.0, 0.0)
            mnext[b] = jnp.where(docpad[9:9 + rows, :] == here, 1.0, 0.0)

    def send_edges(layer):
        for b in range(2):
            edge[layer, b, 0] = mpad[b, 8:24, :].astype(bf)
            edge[layer, b, 1] = mpad[b, rows - 8:rows + 8, :].astype(bf)
        for b in range(2):
            for side in range(2):
                go(lambda b=b, side=side: halo_copy(layer, b, side))

    def convolve(layer):
        for b in range(2):
            for side in range(2):
                halo_wait(layer, b, side)
            mpad[b, 7:8, :] = halo[layer, b, 0, 15:16, :].astype(f32)
            mpad[b, 8 + rows:9 + rows, :] = halo[layer, b, 1, 0:1, :].astype(f32)
            for low in range(0, half, 128):
                lanes = slice(low, low + 128)
                tap = [jnp.where(zl == 0, taps_ref[j, layer:layer + 1, low:low + 128],
                                 taps_ref[j, layer:layer + 1, half + low:half + low + 128]) for j in range(3)]
                for r in range(0, rows, small):
                    before = tap[0] * mpad[b, r + 7:r + 7 + small, lanes]
                    middle = tap[1] * mpad[b, r + 8:r + 8 + small, lanes]
                    after = tap[2] * mpad[b, r + 9:r + 9 + small, lanes]
                    here = slice(r, r + small)
                    total = (jnp.where(mprev[b, here, :] > 0.5, before, 0.0) + middle
                             + jnp.where(mnext[b, here, :] > 0.5, after, 0.0))
                    gated[b, here, lanes] = (cbuf[b, here, lanes].astype(f32) * total).astype(bf)

    def owner_of(dx, dc):
        return lax.rem(x + dx, X) * 2 + lax.rem(c + dc, 2)

    def d_copy(layer, dx, i, tb):
        return remote(dsrc.at[layer, dx, i, tb], drcv.at[layer, dx, i, tb], d_send.at[layer, dx, i, tb],
                      d_recv.at[layer, dx, i, tb], (s, sibling))

    def xs_copy(layer, i, tb):
        return remote(xsrc.at[layer, i, tb], xrcv.at[layer, i, tb], x_send.at[layer, i, tb],
                      x_recv.at[layer, i, tb], (s, across))

    def zs_copy(layer, i):
        return remote(zsrc.at[layer, i], zrcv.at[layer, i], z_send.at[layer, i], z_recv.at[layer, i], (mate, t))

    def sweep(use):
        def step(e, carry):
            use(e // 2, e % 2)
            return carry

        lax.fori_loop(0, 2 * per, step, 0)

    def partial(layer, dx, dc, i, tb):
        shard = owner_of(dx, dc) * per + i
        return jnp.dot(gated[lax.rem(theirs + tb, 2)], wout[layer, shard], preferred_element_type=f32)

    def hand_over(layer, dx):
        def use(i, tb):
            dsrc[layer, dx, i, tb] = partial(layer, dx, 1, i, tb).astype(bf)
            d_copy(layer, dx, i, tb).start()

        sweep(use)

    def send_across(layer):
        def use(i, tb):
            part = partial(layer, 1, 0, i, tb)
            d_copy(layer, 1, i, tb).wait_recv()
            xsrc[layer, i, tb] = (part + drcv[layer, 1, i, tb].astype(f32)).astype(bf)
            xs_copy(layer, i, tb).start()

        sweep(use)

    def hold(layer):
        def use(i, tb):
            part = partial(layer, 0, 0, i, tb)
            d_copy(layer, 0, i, tb).wait_recv()
            acc[i, tb] = part + drcv[layer, 0, i, tb].astype(f32)

        sweep(use)

    def to_mate(layer, i):
        xs_copy(layer, i, 0).wait_recv()
        zsrc[layer, i] = (acc[i, 0] + xrcv[layer, i, 0].astype(f32)).astype(bf)
        go(lambda: zs_copy(layer, i))

    def finish(layer, i):
        xs_copy(layer, i, 1).wait_recv()
        zs_copy(layer, i).wait_recv()
        total = acc[i, 1] + xrcv[layer, i, 1].astype(f32) + zrcv[layer, i].astype(f32)
        fresh = (xfull[layer, zl, t, i].astype(f32) + total).astype(bf)
        if layer + 1 < L:
            xfull[layer + 1, zl, t, i] = fresh
        else:
            result_ref[:, i * ow:(i + 1) * ow] = fresh

    pump(0)
    for layer in range(L):
        base = 4 * layer
        for i in range(per):
            ag_from_z(layer, i)
        if layer == 0:
            masks()
        for i in range(per):
            ag_from_x(layer, zl, i)
        for i in range(per):
            ag_from_x(layer, theirs, i)
        pump(base + 1)
        ag_from_core(layer, zl)
        norm(layer, zl)
        ag_from_core(layer, theirs)
        norm(layer, theirs)
        need(base)
        both(layer, 0, keep_gate)
        pump(base + 2)
        need(base + 1)
        both(layer, 1, mix)
        send_edges(layer)
        need(base + 2)
        both(layer, 2, keep_gate)
        convolve(layer)
        pump(base + 3)
        need(base + 3)
        hand_over(layer, 1)
        send_across(layer)
        hand_over(layer, 0)
        hold(layer)
        pump(base + 4)
        for i in range(per):
            to_mate(layer, i)
        for i in range(per):
            finish(layer, i)
            if layer + 1 < L:
                ag_own(layer + 1, i)

    for copy_of in pending:
        copy_of().wait_send()
    for layer in range(L):
        def drain(i, tb):
            for dx in range(2):
                d_copy(layer, dx, i, tb).wait_send()
            xs_copy(layer, i, tb).wait_send()

        sweep(drain)


def fused(S, T, stream, doc_ids, norm_gain, gate_proj, input_gate, value_proj, taps, out_proj):
    rows, width = stream.shape
    L, depth, cols = gate_proj.shape
    ow = out_proj.shape[2]
    per, half = width // ow, cols // 2
    bf, f32, i32 = jnp.bfloat16, jnp.float32, jnp.int32
    docs = doc_ids.reshape(rows // 128, 128)
    vmem, hbm = pl.BlockSpec(memory_space=pltpu.VMEM), pl.BlockSpec(memory_space=pl.ANY)
    dma = pltpu.SemaphoreType.DMA
    scratch = [
        pltpu.VMEM((3 * L, S * depth, half), bf),
        pltpu.VMEM((L, S, half, ow), bf),
        pltpu.VMEM((3 * L, depth, half), bf),
        pltpu.VMEM((L, half, ow), bf),
        pltpu.VMEM((L, 2, T, per, rows, ow), bf),
        pltpu.VMEM((2, rows, T * width), bf),
        pltpu.VMEM((2, rows, half), bf),
        pltpu.VMEM((2, rows + 16, half), f32),
        pltpu.VMEM((L, 2, 2, 16, half), bf),
        pltpu.VMEM((L, 2, 2, 16, half), bf),
        pltpu.VMEM((S, rows // 128, 128), i32),
        pltpu.VMEM((rows + 16, 128), f32),
        pltpu.VMEM((2, rows, 128), f32),
        pltpu.VMEM((2, rows, 128), f32),
        pltpu.VMEM((2, rows, half), bf),
        pltpu.VMEM((L, 2, per, 2, rows, ow), bf),
        pltpu.VMEM((L, 2, per, 2, rows, ow), bf),
        pltpu.VMEM((L, per, 2, rows, ow), bf),
        pltpu.VMEM((L, per, 2, rows, ow), bf),
        pltpu.VMEM((L, per, rows, ow), bf),
        pltpu.VMEM((L, per, rows, ow), bf),
        pltpu.VMEM((per, 2, rows, ow), f32),
        dma((4 * L, 2)),
        dma((4 * L, S // 2)),
        dma((4 * L, S // 2)),
        dma((4 * L, S)),
        dma((per,)),
        dma((L, per)),
        dma((L, 2, per)),
        dma((L, 2, T, per)),
        dma((L, 2, T, per)),
        dma((L, 2, per, 2)),
        dma((L, 2, per, 2)),
        dma((L, per, 2)),
        dma((L, per, 2)),
        dma((L, per)),
        dma((L, per)),
        dma((L, 2, 2)),
        dma((L, 2, 2)),
        dma((S,)),
        dma((S,)),
    ]
    return pl.pallas_call(
        functools.partial(fused_kernel, S, T, L),
        out_shape=jax.ShapeDtypeStruct((rows, width), bf),
        in_specs=[hbm, vmem, vmem, hbm, hbm, hbm, vmem, hbm],
        out_specs=vmem,
        scratch_shapes=scratch,
        compiler_params=pltpu.CompilerParams(
            collective_id=0, has_side_effects=True, vmem_limit_bytes=60 * 1024 * 1024),
    )(stream, docs, norm_gain, gate_proj, input_gate, value_proj, jnp.transpose(taps, (1, 0, 2)), out_proj)


def solution(mesh):
    sp, tp = mesh.shape["sp"], mesh.shape["tp"]

    def body(*arrays):
        (rows, width), cols, out_width = arrays[0].shape, arrays[3].shape[2], arrays[7].shape[2]
        aligned = out_width % 128 == 0 and cols % 256 == 0 and rows % 128 == 0 and width % out_width == 0
        if aligned and sp % 4 == 0 and tp == 4:
            return fused(sp, tp, *arrays)
        return per_device(*arrays)

    in_specs = (
        P("sp", "tp"),
        P("sp"),
        P(),
        P(None, "sp", "tp"),
        P(None, "sp", "tp"),
        P(None, "sp", "tp"),
        P(None, None, "tp"),
        P(None, "tp", "sp"),
    )
    out_specs = P("sp", "tp")
    return jax.shard_map(
        body, mesh=mesh, in_specs=in_specs, out_specs=out_specs, check_vma=False
    )
```

```python
import functools

import jax
import jax.numpy as jnp
from jax import lax
from jax.experimental import pallas as pl
from jax.experimental.pallas import tpu as pltpu
from jax.sharding import PartitionSpec as P

epsilon = 1e-06


def with_halo(value, sides, width):
    for axis, dim in sides:
        size, length = (lax.axis_size(axis), value.shape[dim])
        up = [(i, (i + 1) % size) for i in range(size - 1)]
        down = [(j, i) for i, j in up]
        last = lax.slice_in_dim(value, length - width, length, axis=dim)
        leading = lax.slice_in_dim(value, 0, width, axis=dim)
        before = lax.ppermute(last, axis, up)
        after = lax.ppermute(leading, axis, down)
        value = jnp.concatenate([before, value, after], axis=dim)
    return value


def per_device(stream, doc_ids, norm_gain, gate_proj, input_gate, value_proj, taps, out_proj):
    layers = gate_proj.shape[0]
    gathered_in = (
        lax.all_gather(gate_proj, "sp", axis=1, tiled=True),
        lax.all_gather(input_gate, "sp", axis=1, tiled=True),
        lax.all_gather(value_proj, "sp", axis=1, tiled=True),
    )
    gathered_out = lax.all_gather(out_proj, "sp", axis=2, tiled=True)
    current = stream
    for layer_index in range(layers):
        full_rows = lax.all_gather(current, "tp", axis=1, tiled=True)
        widened = full_rows.astype(jnp.float32)
        scale = lax.rsqrt(jnp.mean(widened * widened, axis=-1, keepdims=True) + epsilon)
        normed = (widened * scale * norm_gain[layer_index]).astype(jnp.bfloat16)
        gate_b = jnp.dot(normed, gathered_in[0][layer_index], preferred_element_type=jnp.float32)
        gate_c = jnp.dot(normed, gathered_in[1][layer_index], preferred_element_type=jnp.float32)
        values = jnp.dot(normed, gathered_in[2][layer_index], preferred_element_type=jnp.float32)
        gate_b = gate_b.astype(jnp.bfloat16)
        gate_c = gate_c.astype(jnp.bfloat16)
        values = values.astype(jnp.bfloat16)
        mixed_in = (gate_c.astype(jnp.float32) * values.astype(jnp.float32)).astype(jnp.bfloat16)
        padded, doc_padded = (
            with_halo(mixed_in, (("sp", 0),), 1),
            with_halo(doc_ids, (("sp", 0),), 1),
        )
        same_prev = (doc_padded[:-2] == doc_ids)[:, None]
        same_next = (doc_padded[2:] == doc_ids)[:, None]
        kernel_taps = taps[layer_index]
        convolved = (
            jnp.where(same_prev, kernel_taps[0] * padded[:-2].astype(jnp.float32), 0.0)
            + kernel_taps[1] * mixed_in.astype(jnp.float32)
            + jnp.where(same_next, kernel_taps[2] * padded[2:].astype(jnp.float32), 0.0)
        )
        gated = (gate_b.astype(jnp.float32) * convolved).astype(jnp.bfloat16)
        partials = jnp.dot(gated, gathered_out[layer_index], preferred_element_type=jnp.float32)
        summed = lax.psum_scatter(
            partials.astype(jnp.bfloat16), "tp", scatter_dimension=1, tiled=True
        ).astype(jnp.float32)
        current = (current.astype(jnp.float32) + summed).astype(jnp.bfloat16)
    return current


MESH = pl.DeviceIdType.MESH


def fused_kernel(S, T, L, stream_ref, docs_ref, gain_ref, gate_ref, input_ref, value_ref, taps_ref, outw_ref,
                 result_ref, win, wout, stage_in, stage_out, xfull, normed, cbuf, mpad, edge, halo, docall, docpad,
                 mprev, mnext, gated, dsrc, drcv, xsrc, xrcv, zsrc, zrcv, acc,
                 own_sem, w_send, y_send, w_recv, x_sem, agz_send, agx_send, agc_send, ag_recv,
                 d_send, d_recv, x_send, x_recv, z_send, z_recv, h_send, h_recv, doc_send, doc_recv, pace):
    s = lax.axis_index("sp")
    t = lax.axis_index("tp")
    Z = S // 2
    z, y = s // 2, s % 2
    zh, zl = z // 2, z % 2
    x, c = t // 2, t % 2
    X = T // 2
    rows = stream_ref.shape[0]
    depth = gate_ref.shape[1]
    half = taps_ref.shape[2] // 2
    ow = outw_ref.shape[2]
    width = stream_ref.shape[1]
    per = width // ow
    units = 4 * L
    other_y = s + 1 - 2 * y
    sibling = t + 1 - 2 * c
    across = lax.rem(t + 2, T)
    mate = s + 2 - 4 * zl
    theirs = 1 - zl
    sources = (input_ref, value_ref, gate_ref)
    bf, f32 = jnp.bfloat16, jnp.float32
    pending = []

    barrier = pltpu.get_barrier_semaphore()

    def greet(sp_index, tp_index):
        pl.semaphore_signal(barrier, inc=1, device_id=(sp_index, tp_index), device_id_type=MESH)

    for k in range(1, S):
        greet(lax.rem(s + k, S), t)
    greet(s, sibling)
    greet(s, across)

    def remote(src, dst, send_sem, recv_sem, target):
        return pltpu.make_async_remote_copy(src_ref=src, dst_ref=dst, send_sem=send_sem, recv_sem=recv_sem,
                                            device_id=target, device_id_type=MESH)

    def go(copy_of, cond=None):
        if cond is None:
            copy_of().start()
        else:
            pl.when(cond)(lambda: copy_of().start())
        pending.append((copy_of, cond))

    def slot(u, shard):
        layer, part = u // 4, u % 4
        if part < 3:
            return win.at[layer * 3 + part, pl.ds(pl.multiple_of(shard * depth, depth), depth)]
        return wout.at[layer, shard]

    def stage(u):
        layer, part = u // 4, u % 4
        return stage_in.at[layer * 3 + part] if part < 3 else stage_out.at[layer]

    def own_copy(u, which):
        layer, part = u // 4, u % 4
        pick = pl.ds(pl.multiple_of((zl if which == 0 else theirs) * half, half), half)
        source = outw_ref.at[layer, pick, :] if part == 3 else sources[part].at[layer, :, pick]
        return pltpu.make_async_copy(source, slot(u, s) if which == 0 else stage(u), own_sem.at[u, which])

    def piece(layer, plane, owner, i):
        return xfull.at[layer, plane, owner, i]

    def x_copy(i):
        return pltpu.make_async_copy(stream_ref.at[:, i * ow:(i + 1) * ow], piece(0, zl, t, i), x_sem.at[i])

    for i in range(per):
        x_copy(i).start()
    for u in range(units):
        for which in range(2):
            own_copy(u, which).start()

    pl.semaphore_wait(barrier, S + 1)

    def z_copy(u, k):
        plane = lax.rem(z + k, Z)
        return remote(slot(u, s) if k % 2 == 0 else stage(u), slot(u, s), w_send.at[u, k], w_recv.at[u, s],
                      (2 * plane + y, t))

    def y_copy(u, plane):
        shard = 2 * plane + y
        return remote(slot(u, shard), slot(u, shard), y_send.at[u, plane], w_recv.at[u, shard], (other_y, t))

    def own_y(u):
        go(lambda: y_copy(u, z))

    def begin(u):
        for k in range(1, Z):
            go(lambda k=k: z_copy(u, k))

    def arrived(u, shard):
        remote(slot(u, shard), slot(u, shard), y_send.at[u, z], w_recv.at[u, shard], (other_y, t)).wait_recv()

    def pump(u, low=1, high=Z):
        for k in range(low, high):
            plane = lax.rem(z + Z + (2 * zl - 1) * k, Z)
            arrived(u, 2 * plane + y)
            go(lambda plane=plane: y_copy(u, plane))

    def meet(u):
        pl.semaphore_signal(pace.at[u], inc=1, device_id=(s, sibling), device_id_type=MESH)
        pl.semaphore_wait(pace.at[u], 1)

    def need(u):
        for k in range(Z):
            plane = lax.rem(z + k, Z)
            arrived(u, 2 * plane + 1 - y)

    def agz(layer, i):
        return remote(piece(layer, zl, t, i), piece(layer, zl, t, i), agz_send.at[layer, i],
                      ag_recv.at[layer, zl, t, i], (mate, t))

    def agx(layer, plane, i):
        return remote(piece(layer, plane, t, i), piece(layer, plane, t, i), agx_send.at[layer, plane, i],
                      ag_recv.at[layer, plane, t, i], (s, across))

    def agc(layer, plane, owner, i):
        return remote(piece(layer, plane, owner, i), piece(layer, plane, owner, i),
                      agc_send.at[layer, plane, owner, i], ag_recv.at[layer, plane, owner, i], (s, sibling))

    def ag_wait(layer, plane, owner, i):
        remote(piece(layer, plane, owner, i), piece(layer, plane, owner, i), agz_send.at[layer, i],
               ag_recv.at[layer, plane, owner, i], (mate, t)).wait_recv()

    def ag_own(layer, i):
        go(lambda: agz(layer, i))
        go(lambda: agx(layer, zl, i))
        go(lambda: agc(layer, zl, t, i))

    def ag_from_z(layer, i):
        ag_wait(layer, theirs, t, i)
        go(lambda: agx(layer, theirs, i))
        go(lambda: agc(layer, theirs, t, i))

    def ag_from_x(layer, plane, i):
        ag_wait(layer, plane, across, i)
        go(lambda: agc(layer, plane, across, i))

    def ag_from_core(layer, plane):
        for i in range(per):
            ag_wait(layer, plane, sibling, i)
            ag_wait(layer, plane, lax.rem(sibling + 2, T), i)

    def doc_copy(k):
        return remote(docs_ref, docall.at[s], doc_send.at[k], doc_recv.at[s], (lax.rem(s + k, S), t))

    def group_block(b):
        return 2 * (2 * zh + b) + y

    def halo_copy(layer, b, side):
        target = lax.rem(group_block(b) + (1 if side == 0 else S - 1), S)
        core = 2 * (2 * (target // 4) + zl) + target % 2
        return remote(edge.at[layer, b, 1 - side], halo.at[layer, (target // 2) % 2, side],
                      h_send.at[layer, b, side], h_recv.at[layer, (target // 2) % 2, side], (core, t))

    def halo_wait(layer, b, side):
        remote(edge.at[layer, b, side], halo.at[layer, b, side], h_send.at[layer, b, side],
               h_recv.at[layer, b, side], (other_y, t)).wait_recv()

    for k in range(1, S):
        go(lambda k=k: doc_copy(k))
    for i in range(per):
        x_copy(i).wait()
        ag_own(0, i)
    for u in range(units):
        for which in range(2):
            own_copy(u, which).wait()
    for u in range(5):
        own_y(u)
    begin(0)
    begin(1)

    small = rows // 8

    def norm(layer, plane):
        def step(r, carry):
            at = pl.ds(pl.multiple_of(r * small, small), small)
            total = jnp.zeros((small, 1), f32)
            for q in range(T):
                for i in range(per):
                    wide = xfull[layer, plane, q, i, at, :].astype(f32)
                    total = total + jnp.sum(wide * wide, axis=-1, keepdims=True)
            scale = lax.rsqrt(total / (width * T) + epsilon)
            for q in range(T):
                for i in range(per):
                    wide = xfull[layer, plane, q, i, at, :].astype(f32)
                    low = q * width + i * ow
                    gain = gain_ref[layer:layer + 1, low:low + ow]
                    normed[plane, at, low:low + ow] = (wide * scale * gain).astype(bf)
            return carry

        lax.fori_loop(0, rows // small, step, 0)

    def project(layer, part, plane):
        product = jnp.dot(normed[plane], win[layer * 3 + part], preferred_element_type=f32).astype(bf)
        if part == 1:
            mixed = (cbuf[plane].astype(f32) * product.astype(f32)).astype(bf)
            mpad[plane, 8:8 + rows, :] = mixed.astype(f32)
        else:
            cbuf[plane] = product

    def columns(block, row):
        line = docall[block, row:row + 1, :].astype(f32)
        return jnp.transpose(jnp.broadcast_to(line, (128, 128)))

    def masks():
        docall[s] = docs_ref[...]
        for k in range(1, S):
            remote(docs_ref, docall.at[lax.rem(s + k, S)], doc_send.at[k], doc_recv.at[lax.rem(s + k, S)],
                   (other_y, t)).wait_recv()
        lines = rows // 128
        for b in range(2):
            block = group_block(b)
            for j in range(lines):
                docpad[8 + 128 * j:136 + 128 * j, :] = columns(block, j)
            before = columns(lax.rem(block + S - 1, S), lines - 1)[120:128, :]
            after = columns(lax.rem(block + 1, S), 0)[0:8, :]
            docpad[0:8, :] = jnp.where(block > 0, before, -1.0)
            docpad[8 + rows:16 + rows, :] = jnp.where(block < S - 1, after, -1.0)
            here = docpad[8:8 + rows, :]
            mprev[b] = jnp.where(docpad[7:7 + rows, :] == here, 1.0, 0.0)
            mnext[b] = jnp.where(docpad[9:9 + rows, :] == here, 1.0, 0.0)

    def send_edges(layer, b):
        edge[layer, b, 0] = mpad[b, 8:24, :].astype(bf)
        edge[layer, b, 1] = mpad[b, rows - 8:rows + 8, :].astype(bf)
        block = group_block(b)
        go(lambda: halo_copy(layer, b, 0), block < S - 1)
        go(lambda: halo_copy(layer, b, 1), block > 0)

    def convolve(layer):
        for b in range(2):
            block = group_block(b)
            empty = jnp.zeros((1, half), f32)

            @pl.when(block > 0)
            def _():
                halo_wait(layer, b, 0)
                mpad[b, 7:8, :] = halo[layer, b, 0, 15:16, :].astype(f32)

            @pl.when(block == 0)
            def _():
                mpad[b, 7:8, :] = empty

            @pl.when(block < S - 1)
            def _():
                halo_wait(layer, b, 1)
                mpad[b, 8 + rows:9 + rows, :] = halo[layer, b, 1, 0:1, :].astype(f32)

            @pl.when(block == S - 1)
            def _():
                mpad[b, 8 + rows:9 + rows, :] = empty

            for low in range(0, half, 128):
                lanes = slice(low, low + 128)
                tap = [jnp.where(zl == 0, taps_ref[j, layer:layer + 1, low:low + 128],
                                 taps_ref[j, layer:layer + 1, half + low:half + low + 128]) for j in range(3)]
                for r in range(0, rows, small):
                    before = tap[0] * mpad[b, r + 7:r + 7 + small, lanes]
                    middle = tap[1] * mpad[b, r + 8:r + 8 + small, lanes]
                    after = tap[2] * mpad[b, r + 9:r + 9 + small, lanes]
                    here = slice(r, r + small)
                    total = (jnp.where(mprev[b, here, :] > 0.5, before, 0.0) + middle
                             + jnp.where(mnext[b, here, :] > 0.5, after, 0.0))
                    gated[b, here, lanes] = (cbuf[b, here, lanes].astype(f32) * total).astype(bf)

    def owner_of(dx, dc):
        return lax.rem(x + dx, X) * 2 + lax.rem(c + dc, 2)

    def d_copy(layer, dx, i, tb):
        return remote(dsrc.at[layer, dx, i, tb], drcv.at[layer, dx, i, tb], d_send.at[layer, dx, i, tb],
                      d_recv.at[layer, dx, i, tb], (s, sibling))

    def xs_copy(layer, i, tb):
        return remote(xsrc.at[layer, i, tb], xrcv.at[layer, i, tb], x_send.at[layer, i, tb],
                      x_recv.at[layer, i, tb], (s, across))

    def zs_copy(layer, i):
        return remote(zsrc.at[layer, i], zrcv.at[layer, i], z_send.at[layer, i], z_recv.at[layer, i], (mate, t))

    def sweep(use):
        def step(e, carry):
            use(e % per, e // per)
            return carry

        lax.fori_loop(0, 2 * per, step, 0)

    def partial(layer, dx, dc, i, tb):
        shard = owner_of(dx, dc) * per + i
        return jnp.dot(gated[lax.rem(theirs + tb, 2)], wout[layer, shard], preferred_element_type=f32)

    def hand_over(layer, dx):
        def use(i, tb):
            dsrc[layer, dx, i, tb] = partial(layer, dx, 1, i, tb).astype(bf)
            d_copy(layer, dx, i, tb).start()

        sweep(use)

    def send_across(layer):
        def use(i, tb):
            part = partial(layer, 1, 0, i, tb)
            d_copy(layer, 1, i, tb).wait_recv()
            xsrc[layer, i, tb] = (part + drcv[layer, 1, i, tb].astype(f32)).astype(bf)
            xs_copy(layer, i, tb).start()

        sweep(use)

    def hold(layer):
        def use(i, tb):
            part = partial(layer, 0, 0, i, tb)
            d_copy(layer, 0, i, tb).wait_recv()
            acc[i, tb] = part + drcv[layer, 0, i, tb].astype(f32)

        sweep(use)

    def to_mate(layer, i):
        xs_copy(layer, i, 0).wait_recv()
        zsrc[layer, i] = (acc[i, 0] + xrcv[layer, i, 0].astype(f32)).astype(bf)
        go(lambda: zs_copy(layer, i))

    def finish(layer, i):
        xs_copy(layer, i, 1).wait_recv()
        zs_copy(layer, i).wait_recv()
        total = acc[i, 1] + xrcv[layer, i, 1].astype(f32) + zrcv[layer, i].astype(f32)
        fresh = (xfull[layer, zl, t, i].astype(f32) + total).astype(bf)
        if layer + 1 < L:
            xfull[layer + 1, zl, t, i] = fresh
        else:
            result_ref[:, i * ow:(i + 1) * ow] = fresh

    for layer in range(L):
        base = 4 * layer
        last = layer == L - 1
        if layer == 0:
            pump(0, 1, Z - 1)
            for i in range(per):
                ag_from_x(layer, zl, i)
            for i in range(per):
                ag_from_z(layer, i)
            pump(0, Z - 1, Z)
            meet(0)
            begin(2)
            masks()
            pump(1, 1, Z - 1)
            pump(1, Z - 1, Z)
            meet(1)
            begin(3)
        else:
            pump(base + 2)
            for i in range(per):
                ag_from_z(layer, i)
                ag_from_x(layer, zl, i)
        ag_from_core(layer, zl)
        norm(layer, zl)
        need(base)
        project(layer, 0, zl)
        if layer == 0:
            pump(2, 1, Z - 1)
        need(base + 1)
        project(layer, 1, zl)
        send_edges(layer, zl)
        if layer == 0:
            pump(2, Z - 1, Z)
        else:
            pump(base + 3)
            need(base + 2)
            project(layer, 2, zl)
        for i in range(per):
            ag_from_x(layer, theirs, i)
        ag_from_core(layer, theirs)
        norm(layer, theirs)
        project(layer, 0, theirs)
        project(layer, 1, theirs)
        send_edges(layer, theirs)
        if not last:
            begin(base + 4)
        if layer == 0:
            pump(3, 1, Z - 1)
            need(base + 2)
            project(layer, 2, zl)
        project(layer, 2, theirs)
        if layer == 0:
            pump(3, Z - 1, Z)
        if not last:
            meet(base + 3)
            begin(base + 5)
        convolve(layer)
        need(base + 3)
        if not last:
            for u in range(base + 5, base + 8):
                own_y(u)
        hand_over(layer, 1)
        send_across(layer)
        hand_over(layer, 0)
        hold(layer)
        if not last:
            pump(base + 4)
        for i in range(per):
            to_mate(layer, i)
        if not last:
            begin(base + 6)
            pump(base + 5)
        for i in range(per):
            finish(layer, i)
            if not last:
                ag_own(layer + 1, i)
        if not last:
            begin(base + 7)

    for copy_of, cond in pending:
        if cond is None:
            copy_of().wait_send()
        else:
            pl.when(cond)(lambda copy_of=copy_of: copy_of().wait_send())
    for layer in range(L):
        def drain(i, tb):
            for dx in range(2):
                d_copy(layer, dx, i, tb).wait_send()
            xs_copy(layer, i, tb).wait_send()

        sweep(drain)


def fused(S, T, stream, doc_ids, norm_gain, gate_proj, input_gate, value_proj, taps, out_proj):
    rows, width = stream.shape
    L, depth, cols = gate_proj.shape
    ow = out_proj.shape[2]
    per, half = width // ow, cols // 2
    bf, f32, i32 = jnp.bfloat16, jnp.float32, jnp.int32
    docs = doc_ids.reshape(rows // 128, 128)
    vmem, hbm = pl.BlockSpec(memory_space=pltpu.VMEM), pl.BlockSpec(memory_space=pl.ANY)
    dma = pltpu.SemaphoreType.DMA
    scratch = [
        pltpu.VMEM((3 * L, S * depth, half), bf),
        pltpu.VMEM((L, S, half, ow), bf),
        pltpu.VMEM((3 * L, depth, half), bf),
        pltpu.VMEM((L, half, ow), bf),
        pltpu.VMEM((L, 2, T, per, rows, ow), bf),
        pltpu.VMEM((2, rows, T * width), bf),
        pltpu.VMEM((2, rows, half), bf),
        pltpu.VMEM((2, rows + 16, half), f32),
        pltpu.VMEM((L, 2, 2, 16, half), bf),
        pltpu.VMEM((L, 2, 2, 16, half), bf),
        pltpu.VMEM((S, rows // 128, 128), i32),
        pltpu.VMEM((rows + 16, 128), f32),
        pltpu.VMEM((2, rows, 128), f32),
        pltpu.VMEM((2, rows, 128), f32),
        pltpu.VMEM((2, rows, half), bf),
        pltpu.VMEM((L, 2, per, 2, rows, ow), bf),
        pltpu.VMEM((L, 2, per, 2, rows, ow), bf),
        pltpu.VMEM((L, per, 2, rows, ow), bf),
        pltpu.VMEM((L, per, 2, rows, ow), bf),
        pltpu.VMEM((L, per, rows, ow), bf),
        pltpu.VMEM((L, per, rows, ow), bf),
        pltpu.VMEM((per, 2, rows, ow), f32),
        dma((4 * L, 2)),
        dma((4 * L, S // 2)),
        dma((4 * L, S // 2)),
        dma((4 * L, S)),
        dma((per,)),
        dma((L, per)),
        dma((L, 2, per)),
        dma((L, 2, T, per)),
        dma((L, 2, T, per)),
        dma((L, 2, per, 2)),
        dma((L, 2, per, 2)),
        dma((L, per, 2)),
        dma((L, per, 2)),
        dma((L, per)),
        dma((L, per)),
        dma((L, 2, 2)),
        dma((L, 2, 2)),
        dma((S,)),
        dma((S,)),
        pltpu.SemaphoreType.REGULAR((4 * L,)),
    ]
    return pl.pallas_call(
        functools.partial(fused_kernel, S, T, L),
        out_shape=jax.ShapeDtypeStruct((rows, width), bf),
        in_specs=[hbm, vmem, vmem, hbm, hbm, hbm, vmem, hbm],
        out_specs=vmem,
        scratch_shapes=scratch,
        compiler_params=pltpu.CompilerParams(
            collective_id=0, has_side_effects=True, vmem_limit_bytes=60 * 1024 * 1024),
    )(stream, docs, norm_gain, gate_proj, input_gate, value_proj, jnp.transpose(taps, (1, 0, 2)), out_proj)


def solution(mesh):
    sp, tp = mesh.shape["sp"], mesh.shape["tp"]

    def body(*arrays):
        (rows, width), cols, out_width = arrays[0].shape, arrays[3].shape[2], arrays[7].shape[2]
        aligned = out_width % 128 == 0 and cols % 256 == 0 and rows % 128 == 0 and width % out_width == 0
        if aligned and sp % 4 == 0 and tp == 4:
            return fused(sp, tp, *arrays)
        return per_device(*arrays)

    in_specs = (
        P("sp", "tp"),
        P("sp"),
        P(),
        P(None, "sp", "tp"),
        P(None, "sp", "tp"),
        P(None, "sp", "tp"),
        P(None, None, "tp"),
        P(None, "tp", "sp"),
    )
    out_specs = P("sp", "tp")
    return jax.shard_map(
        body, mesh=mesh, in_specs=in_specs, out_specs=out_specs, check_vma=False
    )
```

```python
import functools

import jax
import jax.numpy as jnp
from jax import lax
from jax.experimental import pallas as pl
from jax.experimental.pallas import tpu as pltpu
from jax.sharding import PartitionSpec as P

epsilon = 1e-06


def with_halo(value, sides, width):
    for axis, dim in sides:
        size, length = (lax.axis_size(axis), value.shape[dim])
        up = [(i, (i + 1) % size) for i in range(size - 1)]
        down = [(j, i) for i, j in up]
        last = lax.slice_in_dim(value, length - width, length, axis=dim)
        leading = lax.slice_in_dim(value, 0, width, axis=dim)
        before = lax.ppermute(last, axis, up)
        after = lax.ppermute(leading, axis, down)
        value = jnp.concatenate([before, value, after], axis=dim)
    return value


def per_device(stream, doc_ids, norm_gain, gate_proj, input_gate, value_proj, taps, out_proj):
    layers = gate_proj.shape[0]
    gathered_in = (
        lax.all_gather(gate_proj, "sp", axis=1, tiled=True),
        lax.all_gather(input_gate, "sp", axis=1, tiled=True),
        lax.all_gather(value_proj, "sp", axis=1, tiled=True),
    )
    gathered_out = lax.all_gather(out_proj, "sp", axis=2, tiled=True)
    current = stream
    for layer_index in range(layers):
        full_rows = lax.all_gather(current, "tp", axis=1, tiled=True)
        widened = full_rows.astype(jnp.float32)
        scale = lax.rsqrt(jnp.mean(widened * widened, axis=-1, keepdims=True) + epsilon)
        normed = (widened * scale * norm_gain[layer_index]).astype(jnp.bfloat16)
        gate_b = jnp.dot(normed, gathered_in[0][layer_index], preferred_element_type=jnp.float32)
        gate_c = jnp.dot(normed, gathered_in[1][layer_index], preferred_element_type=jnp.float32)
        values = jnp.dot(normed, gathered_in[2][layer_index], preferred_element_type=jnp.float32)
        gate_b = gate_b.astype(jnp.bfloat16)
        gate_c = gate_c.astype(jnp.bfloat16)
        values = values.astype(jnp.bfloat16)
        mixed_in = (gate_c.astype(jnp.float32) * values.astype(jnp.float32)).astype(jnp.bfloat16)
        padded, doc_padded = (
            with_halo(mixed_in, (("sp", 0),), 1),
            with_halo(doc_ids, (("sp", 0),), 1),
        )
        same_prev = (doc_padded[:-2] == doc_ids)[:, None]
        same_next = (doc_padded[2:] == doc_ids)[:, None]
        kernel_taps = taps[layer_index]
        convolved = (
            jnp.where(same_prev, kernel_taps[0] * padded[:-2].astype(jnp.float32), 0.0)
            + kernel_taps[1] * mixed_in.astype(jnp.float32)
            + jnp.where(same_next, kernel_taps[2] * padded[2:].astype(jnp.float32), 0.0)
        )
        gated = (gate_b.astype(jnp.float32) * convolved).astype(jnp.bfloat16)
        partials = jnp.dot(gated, gathered_out[layer_index], preferred_element_type=jnp.float32)
        summed = lax.psum_scatter(
            partials.astype(jnp.bfloat16), "tp", scatter_dimension=1, tiled=True
        ).astype(jnp.float32)
        current = (current.astype(jnp.float32) + summed).astype(jnp.bfloat16)
    return current


MESH = pl.DeviceIdType.MESH


def fused_kernel(S, T, L, stream_ref, docs_ref, gain_ref, gate_ref, input_ref, value_ref, taps_ref, outw_ref,
                 result_ref, win, wout, stage_in, stage_out, xfull, normed, cbuf, mpad, edge, halo, docall, docpad,
                 mprev, mnext, gated, dsrc, drcv, xsrc, xrcv, zsrc, zrcv, acc, zqsrc, zqrcv, xqsrc, xqrcv, accq,
                 own_sem, w_send, y_send, w_recv, x_sem, agz_send, agx_send, agc_send, ag_recv,
                 d_send, d_recv, x_send, x_recv, z_send, z_recv, h_send, h_recv, doc_send, doc_recv, pace,
                 zq_send, zq_recv, xq_send, xq_recv):
    s = lax.axis_index("sp")
    t = lax.axis_index("tp")
    Z = S // 2
    z, y = s // 2, s % 2
    zh, zl = z // 2, z % 2
    x, c = t // 2, t % 2
    X = T // 2
    rows = stream_ref.shape[0]
    depth = gate_ref.shape[1]
    half = taps_ref.shape[2] // 2
    ow = outw_ref.shape[2]
    width = stream_ref.shape[1]
    per = width // ow
    units = 4 * L
    other_y = s + 1 - 2 * y
    sibling = t + 1 - 2 * c
    across = lax.rem(t + 2, T)
    mate = s + 2 - 4 * zl
    theirs = 1 - zl
    sources = (input_ref, value_ref, gate_ref)
    bf, f32 = jnp.bfloat16, jnp.float32
    pending = []

    barrier = pltpu.get_barrier_semaphore()

    def greet(sp_index, tp_index):
        pl.semaphore_signal(barrier, inc=1, device_id=(sp_index, tp_index), device_id_type=MESH)

    for k in range(1, S):
        greet(lax.rem(s + k, S), t)
    greet(s, sibling)
    greet(s, across)

    def remote(src, dst, send_sem, recv_sem, target):
        return pltpu.make_async_remote_copy(src_ref=src, dst_ref=dst, send_sem=send_sem, recv_sem=recv_sem,
                                            device_id=target, device_id_type=MESH)

    def go(copy_of, cond=None):
        if cond is None:
            copy_of().start()
        else:
            pl.when(cond)(lambda: copy_of().start())
        pending.append((copy_of, cond))

    def slot(u, shard):
        layer, part = u // 4, u % 4
        if part < 3:
            return win.at[layer * 3 + part, pl.ds(pl.multiple_of(shard * depth, depth), depth)]
        return wout.at[layer, shard]

    def stage(u):
        layer, part = u // 4, u % 4
        return stage_in.at[layer * 3 + part] if part < 3 else stage_out.at[layer]

    def own_copy(u, which):
        layer, part = u // 4, u % 4
        pick = pl.ds(pl.multiple_of((zl if which == 0 else theirs) * half, half), half)
        source = outw_ref.at[layer, pick, :] if part == 3 else sources[part].at[layer, :, pick]
        return pltpu.make_async_copy(source, slot(u, s) if which == 0 else stage(u), own_sem.at[u, which])

    def piece(layer, plane, owner, i):
        return xfull.at[layer, plane, owner, i]

    def x_copy(i):
        return pltpu.make_async_copy(stream_ref.at[:, i * ow:(i + 1) * ow], piece(0, zl, t, i), x_sem.at[i])

    for i in range(per):
        x_copy(i).start()
    for u in range(units):
        for which in range(2):
            own_copy(u, which).start()

    pl.semaphore_wait(barrier, S + 1)

    def z_copy(u, k):
        plane = lax.rem(z + k, Z)
        return remote(slot(u, s) if k % 2 == 0 else stage(u), slot(u, s), w_send.at[u, k], w_recv.at[u, s],
                      (2 * plane + y, t))

    def y_copy(u, plane):
        shard = 2 * plane + y
        return remote(slot(u, shard), slot(u, shard), y_send.at[u, plane], w_recv.at[u, shard], (other_y, t))

    def own_y(u):
        go(lambda: y_copy(u, z))

    def begin(u):
        for k in range(1, Z):
            go(lambda k=k: z_copy(u, k))

    def arrived(u, shard):
        remote(slot(u, shard), slot(u, shard), y_send.at[u, z], w_recv.at[u, shard], (other_y, t)).wait_recv()

    def pump(u, low=1, high=Z):
        for k in range(low, high):
            plane = lax.rem(z + Z + (2 * zl - 1) * k, Z)
            arrived(u, 2 * plane + y)
            go(lambda plane=plane: y_copy(u, plane))

    def meet(u):
        pl.semaphore_signal(pace.at[u], inc=1, device_id=(s, sibling), device_id_type=MESH)
        pl.semaphore_wait(pace.at[u], 1)

    def need(u):
        for k in range(Z):
            plane = lax.rem(z + k, Z)
            arrived(u, 2 * plane + 1 - y)

    def agz(layer, i):
        return remote(piece(layer, zl, t, i), piece(layer, zl, t, i), agz_send.at[layer, i],
                      ag_recv.at[layer, zl, t, i], (mate, t))

    def agx(layer, plane, i):
        return remote(piece(layer, plane, t, i), piece(layer, plane, t, i), agx_send.at[layer, plane, i],
                      ag_recv.at[layer, plane, t, i], (s, across))

    def agc(layer, plane, owner, i):
        return remote(piece(layer, plane, owner, i), piece(layer, plane, owner, i),
                      agc_send.at[layer, plane, owner, i], ag_recv.at[layer, plane, owner, i], (s, sibling))

    def ag_wait(layer, plane, owner, i):
        remote(piece(layer, plane, owner, i), piece(layer, plane, owner, i), agz_send.at[layer, i],
               ag_recv.at[layer, plane, owner, i], (mate, t)).wait_recv()

    def ag_own(layer, i):
        go(lambda: agz(layer, i))
        go(lambda: agx(layer, zl, i))
        go(lambda: agc(layer, zl, t, i))

    def ag_from_z(layer, i):
        ag_wait(layer, theirs, t, i)
        go(lambda: agx(layer, theirs, i))
        go(lambda: agc(layer, theirs, t, i))

    def ag_from_x(layer, plane, i):
        ag_wait(layer, plane, across, i)
        go(lambda: agc(layer, plane, across, i))

    def ag_from_core(layer, plane):
        for i in range(per):
            ag_wait(layer, plane, sibling, i)
            ag_wait(layer, plane, lax.rem(sibling + 2, T), i)

    def doc_copy(k):
        return remote(docs_ref, docall.at[s], doc_send.at[k], doc_recv.at[s], (lax.rem(s + k, S), t))

    def group_block(b):
        return 2 * (2 * zh + b) + y

    def halo_copy(layer, b, side):
        target = lax.rem(group_block(b) + (1 if side == 0 else S - 1), S)
        core = 2 * (2 * (target // 4) + zl) + target % 2
        return remote(edge.at[layer, b, 1 - side], halo.at[layer, (target // 2) % 2, side],
                      h_send.at[layer, b, side], h_recv.at[layer, (target // 2) % 2, side], (core, t))

    def halo_wait(layer, b, side):
        remote(edge.at[layer, b, side], halo.at[layer, b, side], h_send.at[layer, b, side],
               h_recv.at[layer, b, side], (other_y, t)).wait_recv()

    for k in range(1, S):
        go(lambda k=k: doc_copy(k))
    for i in range(per):
        x_copy(i).wait()
        ag_own(0, i)
    for u in range(units):
        for which in range(2):
            own_copy(u, which).wait()
    for u in range(4):
        own_y(u)
    begin(0)
    begin(1)

    small = rows // 8

    def norm(layer, plane):
        def step(r, carry):
            at = pl.ds(pl.multiple_of(r * small, small), small)
            total = jnp.zeros((small, 1), f32)
            for q in range(T):
                for i in range(per):
                    wide = xfull[layer, plane, q, i, at, :].astype(f32)
                    total = total + jnp.sum(wide * wide, axis=-1, keepdims=True)
            scale = lax.rsqrt(total / (width * T) + epsilon)
            for q in range(T):
                for i in range(per):
                    wide = xfull[layer, plane, q, i, at, :].astype(f32)
                    low = q * width + i * ow
                    gain = gain_ref[layer:layer + 1, low:low + ow]
                    normed[plane, at, low:low + ow] = (wide * scale * gain).astype(bf)
            return carry

        lax.fori_loop(0, rows // small, step, 0)

    def project(layer, part, plane):
        product = jnp.dot(normed[plane], win[layer * 3 + part], preferred_element_type=f32).astype(bf)
        if part == 1:
            mixed = (cbuf[plane].astype(f32) * product.astype(f32)).astype(bf)
            mpad[plane, 8:8 + rows, :] = mixed.astype(f32)
        else:
            cbuf[plane] = product

    def columns(block, row):
        line = docall[block, row:row + 1, :].astype(f32)
        return jnp.transpose(jnp.broadcast_to(line, (128, 128)))

    def masks():
        docall[s] = docs_ref[...]
        for k in range(1, S):
            remote(docs_ref, docall.at[lax.rem(s + k, S)], doc_send.at[k], doc_recv.at[lax.rem(s + k, S)],
                   (other_y, t)).wait_recv()
        lines = rows // 128
        for b in range(2):
            block = group_block(b)
            for j in range(lines):
                docpad[8 + 128 * j:136 + 128 * j, :] = columns(block, j)
            before = columns(lax.rem(block + S - 1, S), lines - 1)[120:128, :]
            after = columns(lax.rem(block + 1, S), 0)[0:8, :]
            docpad[0:8, :] = jnp.where(block > 0, before, -1.0)
            docpad[8 + rows:16 + rows, :] = jnp.where(block < S - 1, after, -1.0)
            here = docpad[8:8 + rows, :]
            mprev[b] = jnp.where(docpad[7:7 + rows, :] == here, 1.0, 0.0)
            mnext[b] = jnp.where(docpad[9:9 + rows, :] == here, 1.0, 0.0)

    def send_edges(layer, b):
        edge[layer, b, 0] = mpad[b, 8:24, :].astype(bf)
        edge[layer, b, 1] = mpad[b, rows - 8:rows + 8, :].astype(bf)
        block = group_block(b)
        go(lambda: halo_copy(layer, b, 0), block < S - 1)
        go(lambda: halo_copy(layer, b, 1), block > 0)

    def convolve(layer):
        for b in range(2):
            block = group_block(b)
            empty = jnp.zeros((1, half), f32)

            @pl.when(block > 0)
            def _():
                halo_wait(layer, b, 0)
                mpad[b, 7:8, :] = halo[layer, b, 0, 15:16, :].astype(f32)

            @pl.when(block == 0)
            def _():
                mpad[b, 7:8, :] = empty

            @pl.when(block < S - 1)
            def _():
                halo_wait(layer, b, 1)
                mpad[b, 8 + rows:9 + rows, :] = halo[layer, b, 1, 0:1, :].astype(f32)

            @pl.when(block == S - 1)
            def _():
                mpad[b, 8 + rows:9 + rows, :] = empty

            for low in range(0, half, 128):
                lanes = slice(low, low + 128)
                tap = [jnp.where(zl == 0, taps_ref[j, layer:layer + 1, low:low + 128],
                                 taps_ref[j, layer:layer + 1, half + low:half + low + 128]) for j in range(3)]
                for r in range(0, rows, small):
                    before = tap[0] * mpad[b, r + 7:r + 7 + small, lanes]
                    middle = tap[1] * mpad[b, r + 8:r + 8 + small, lanes]
                    after = tap[2] * mpad[b, r + 9:r + 9 + small, lanes]
                    here = slice(r, r + small)
                    total = (jnp.where(mprev[b, here, :] > 0.5, before, 0.0) + middle
                             + jnp.where(mnext[b, here, :] > 0.5, after, 0.0))
                    gated[b, here, lanes] = (cbuf[b, here, lanes].astype(f32) * total).astype(bf)

    def owner_of(dx, dc):
        return lax.rem(x + dx, X) * 2 + lax.rem(c + dc, 2)

    def d_copy(layer, dx, i, tb):
        return remote(dsrc.at[layer, dx, i, tb], drcv.at[layer, dx, i, tb], d_send.at[layer, dx, i, tb],
                      d_recv.at[layer, dx, i, tb], (s, sibling))

    def xs_copy(layer, i, tb):
        return remote(xsrc.at[layer, i, tb], xrcv.at[layer, i, tb], x_send.at[layer, i, tb],
                      x_recv.at[layer, i, tb], (s, across))

    def zs_copy(layer, i):
        return remote(zsrc.at[layer, i], zrcv.at[layer, i], z_send.at[layer, i], z_recv.at[layer, i], (mate, t))

    def sweep(use):
        def step(e, carry):
            use(e % per, e // per)
            return carry

        lax.fori_loop(0, 2 * per, step, 0)

    def partial(layer, dx, dc, i, tb):
        shard = owner_of(dx, dc) * per + i
        return jnp.dot(gated[lax.rem(theirs + tb, 2)], wout[layer, shard], preferred_element_type=f32)

    def hand_over(layer, dx):
        def use(i, tb):
            dsrc[layer, dx, i, tb] = partial(layer, dx, 1, i, tb).astype(bf)
            d_copy(layer, dx, i, tb).start()

        sweep(use)

    def send_across(layer):
        def use(i, tb):
            part = partial(layer, 1, 0, i, tb)
            d_copy(layer, 1, i, tb).wait_recv()
            xsrc[layer, i, tb] = (part + drcv[layer, 1, i, tb].astype(f32)).astype(bf)
            xs_copy(layer, i, tb).start()

        sweep(use)

    def hold(layer):
        def use(i, tb):
            part = partial(layer, 0, 0, i, tb)
            d_copy(layer, 0, i, tb).wait_recv()
            acc[i, tb] = part + drcv[layer, 0, i, tb].astype(f32)

        sweep(use)

    def joined(layer, dx, i, tb):
        part = partial(layer, dx, 0, i, tb)
        d_copy(layer, dx, i, tb).wait_recv()
        return part + drcv[layer, dx, i, tb].astype(f32)

    tail = per - 1

    def zq_copy(dx):
        return remote(zqsrc.at[dx], zqrcv.at[dx], zq_send.at[dx], zq_recv.at[dx], (mate, t))

    def xq_copy():
        return remote(xqsrc, xqrcv, xq_send, xq_recv, (s, across))

    def to_mate_first(layer, dx):
        zqsrc[dx] = joined(layer, dx, tail, 0).astype(bf)
        go(lambda: zq_copy(dx))

    def send_both(layer):
        to_mate_first(layer, 1)
        for tb in range(2):
            for i in range(tail):
                xsrc[layer, i, tb] = joined(layer, 1, i, tb).astype(bf)
                go(lambda i=i, tb=tb: xs_copy(layer, i, tb))
        accq[...] = joined(layer, 1, tail, 1)

    def hold_both(layer):
        to_mate_first(layer, 0)
        for tb in range(2):
            for i in range(tail):
                acc[i, tb] = joined(layer, 0, i, tb)
        acc[tail, 1] = joined(layer, 0, tail, 1)

    def cross_sum():
        zq_copy(1).wait_recv()
        xqsrc[...] = (accq[...] + zqrcv[1].astype(f32)).astype(bf)
        go(xq_copy)

    def finish_crossed(layer):
        zq_copy(0).wait_recv()
        xq_copy().wait_recv()
        total = acc[tail, 1] + zqrcv[0].astype(f32) + xqrcv[...].astype(f32)
        fresh = (xfull[layer, zl, t, tail].astype(f32) + total).astype(bf)
        result_ref[:, tail * ow:(tail + 1) * ow] = fresh

    def to_mate(layer, i):
        xs_copy(layer, i, 0).wait_recv()
        zsrc[layer, i] = (acc[i, 0] + xrcv[layer, i, 0].astype(f32)).astype(bf)
        go(lambda: zs_copy(layer, i))

    def finish(layer, i):
        xs_copy(layer, i, 1).wait_recv()
        zs_copy(layer, i).wait_recv()
        total = acc[i, 1] + xrcv[layer, i, 1].astype(f32) + zrcv[layer, i].astype(f32)
        fresh = (xfull[layer, zl, t, i].astype(f32) + total).astype(bf)
        if layer + 1 < L:
            xfull[layer + 1, zl, t, i] = fresh
        else:
            result_ref[:, i * ow:(i + 1) * ow] = fresh

    for layer in range(L):
        base = 4 * layer
        last = layer == L - 1
        if layer == 0:
            pump(0, 1, Z - 1)
            meet(0)
            begin(2)
            for i in range(per):
                ag_from_x(layer, zl, i)
            for i in range(per):
                ag_from_z(layer, i)
            pump(0, Z - 1, Z)
            masks()
            pump(1)
            meet(1)
            begin(3)
        else:
            pump(base + 2)
            ag_from_z(layer, 0)
            for i in range(per):
                ag_from_x(layer, zl, i)
        ag_from_core(layer, zl)
        norm(layer, zl)
        if layer > 0:
            for i in range(1, per):
                ag_from_z(layer, i)
        need(base)
        project(layer, 0, zl)
        if layer == 0:
            pump(2, 1, Z - 1)
        need(base + 1)
        project(layer, 1, zl)
        send_edges(layer, zl)
        if layer == 0:
            pump(2, Z - 1, Z)
        else:
            pump(base + 3)
        for i in range(per):
            ag_from_x(layer, theirs, i)
        ag_from_core(layer, theirs)
        norm(layer, theirs)
        project(layer, 0, theirs)
        project(layer, 1, theirs)
        send_edges(layer, theirs)
        if layer == 0:
            pump(3)
        if not last:
            begin(base + 4)
        need(base + 2)
        project(layer, 2, zl)
        project(layer, 2, theirs)
        if not last:
            meet(base + 3)
            begin(base + 5)
        convolve(layer)
        need(base + 3)
        if not last:
            begin(base + 6)
            for u in range(base + 4, base + 8):
                own_y(u)
        hand_over(layer, 1)
        if last:
            send_both(layer)
        else:
            send_across(layer)
        hand_over(layer, 0)
        if last:
            hold_both(layer)
        else:
            hold(layer)
        if not last:
            pump(base + 4)
        for i in range(per - 1 if last else per):
            to_mate(layer, i)
        if last:
            cross_sum()
        else:
            pump(base + 5)
        for i in range(per - 1 if last else per):
            finish(layer, i)
            if not last:
                ag_own(layer + 1, i)
        if last:
            finish_crossed(layer)
        else:
            begin(base + 7)

    for copy_of, cond in pending:
        if cond is None:
            copy_of().wait_send()
        else:
            pl.when(cond)(lambda copy_of=copy_of: copy_of().wait_send())
    for layer in range(L):
        def drain(i, tb):
            for dx in range(2):
                d_copy(layer, dx, i, tb).wait_send()
            if layer + 1 < L:
                xs_copy(layer, i, tb).wait_send()

        sweep(drain)


def fused(S, T, stream, doc_ids, norm_gain, gate_proj, input_gate, value_proj, taps, out_proj):
    rows, width = stream.shape
    L, depth, cols = gate_proj.shape
    ow = out_proj.shape[2]
    per, half = width // ow, cols // 2
    bf, f32, i32 = jnp.bfloat16, jnp.float32, jnp.int32
    docs = doc_ids.reshape(rows // 128, 128)
    vmem, hbm = pl.BlockSpec(memory_space=pltpu.VMEM), pl.BlockSpec(memory_space=pl.ANY)
    dma = pltpu.SemaphoreType.DMA
    scratch = [
        pltpu.VMEM((3 * L, S * depth, half), bf),
        pltpu.VMEM((L, S, half, ow), bf),
        pltpu.VMEM((3 * L, depth, half), bf),
        pltpu.VMEM((L, half, ow), bf),
        pltpu.VMEM((L, 2, T, per, rows, ow), bf),
        pltpu.VMEM((2, rows, T * width), bf),
        pltpu.VMEM((2, rows, half), bf),
        pltpu.VMEM((2, rows + 16, half), f32),
        pltpu.VMEM((L, 2, 2, 16, half), bf),
        pltpu.VMEM((L, 2, 2, 16, half), bf),
        pltpu.VMEM((S, rows // 128, 128), i32),
        pltpu.VMEM((rows + 16, 128), f32),
        pltpu.VMEM((2, rows, 128), f32),
        pltpu.VMEM((2, rows, 128), f32),
        pltpu.VMEM((2, rows, half), bf),
        pltpu.VMEM((L, 2, per, 2, rows, ow), bf),
        pltpu.VMEM((L, 2, per, 2, rows, ow), bf),
        pltpu.VMEM((L, per, 2, rows, ow), bf),
        pltpu.VMEM((L, per, 2, rows, ow), bf),
        pltpu.VMEM((L, per, rows, ow), bf),
        pltpu.VMEM((L, per, rows, ow), bf),
        pltpu.VMEM((per, 2, rows, ow), f32),
        pltpu.VMEM((2, rows, ow), bf),
        pltpu.VMEM((2, rows, ow), bf),
        pltpu.VMEM((rows, ow), bf),
        pltpu.VMEM((rows, ow), bf),
        pltpu.VMEM((rows, ow), f32),
        dma((4 * L, 2)),
        dma((4 * L, S // 2)),
        dma((4 * L, S // 2)),
        dma((4 * L, S)),
        dma((per,)),
        dma((L, per)),
        dma((L, 2, per)),
        dma((L, 2, T, per)),
        dma((L, 2, T, per)),
        dma((L, 2, per, 2)),
        dma((L, 2, per, 2)),
        dma((L, per, 2)),
        dma((L, per, 2)),
        dma((L, per)),
        dma((L, per)),
        dma((L, 2, 2)),
        dma((L, 2, 2)),
        dma((S,)),
        dma((S,)),
        pltpu.SemaphoreType.REGULAR((4 * L,)),
        dma((2,)),
        dma((2,)),
        dma,
        dma,
    ]
    return pl.pallas_call(
        functools.partial(fused_kernel, S, T, L),
        out_shape=jax.ShapeDtypeStruct((rows, width), bf),
        in_specs=[hbm, vmem, vmem, hbm, hbm, hbm, vmem, hbm],
        out_specs=vmem,
        scratch_shapes=scratch,
        compiler_params=pltpu.CompilerParams(
            collective_id=0, has_side_effects=True, vmem_limit_bytes=60 * 1024 * 1024),
    )(stream, docs, norm_gain, gate_proj, input_gate, value_proj, jnp.transpose(taps, (1, 0, 2)), out_proj)


def solution(mesh):
    sp, tp = mesh.shape["sp"], mesh.shape["tp"]

    def body(*arrays):
        (rows, width), cols, out_width = arrays[0].shape, arrays[3].shape[2], arrays[7].shape[2]
        aligned = out_width % 128 == 0 and cols % 256 == 0 and rows % 128 == 0 and width % out_width == 0
        if aligned and sp % 4 == 0 and tp == 4:
            return fused(sp, tp, *arrays)
        return per_device(*arrays)

    in_specs = (
        P("sp", "tp"),
        P("sp"),
        P(),
        P(None, "sp", "tp"),
        P(None, "sp", "tp"),
        P(None, "sp", "tp"),
        P(None, None, "tp"),
        P(None, "tp", "sp"),
    )
    out_specs = P("sp", "tp")
    return jax.shard_map(
        body, mesh=mesh, in_specs=in_specs, out_specs=out_specs, check_vma=False
    )
```

```python
import functools

import jax
import jax.numpy as jnp
from jax import lax
from jax.experimental import pallas as pl
from jax.experimental.pallas import tpu as pltpu
from jax.sharding import PartitionSpec as P

epsilon = 1e-06


def with_halo(value, sides, width):
    for axis, dim in sides:
        size, length = (lax.axis_size(axis), value.shape[dim])
        up = [(i, (i + 1) % size) for i in range(size - 1)]
        down = [(j, i) for i, j in up]
        last = lax.slice_in_dim(value, length - width, length, axis=dim)
        leading = lax.slice_in_dim(value, 0, width, axis=dim)
        before = lax.ppermute(last, axis, up)
        after = lax.ppermute(leading, axis, down)
        value = jnp.concatenate([before, value, after], axis=dim)
    return value


def per_device(stream, doc_ids, norm_gain, gate_proj, input_gate, value_proj, taps, out_proj):
    layers = gate_proj.shape[0]
    gathered_in = (
        lax.all_gather(gate_proj, "sp", axis=1, tiled=True),
        lax.all_gather(input_gate, "sp", axis=1, tiled=True),
        lax.all_gather(value_proj, "sp", axis=1, tiled=True),
    )
    gathered_out = lax.all_gather(out_proj, "sp", axis=2, tiled=True)
    current = stream
    for layer_index in range(layers):
        full_rows = lax.all_gather(current, "tp", axis=1, tiled=True)
        widened = full_rows.astype(jnp.float32)
        scale = lax.rsqrt(jnp.mean(widened * widened, axis=-1, keepdims=True) + epsilon)
        normed = (widened * scale * norm_gain[layer_index]).astype(jnp.bfloat16)
        gate_b = jnp.dot(normed, gathered_in[0][layer_index], preferred_element_type=jnp.float32)
        gate_c = jnp.dot(normed, gathered_in[1][layer_index], preferred_element_type=jnp.float32)
        values = jnp.dot(normed, gathered_in[2][layer_index], preferred_element_type=jnp.float32)
        gate_b = gate_b.astype(jnp.bfloat16)
        gate_c = gate_c.astype(jnp.bfloat16)
        values = values.astype(jnp.bfloat16)
        mixed_in = (gate_c.astype(jnp.float32) * values.astype(jnp.float32)).astype(jnp.bfloat16)
        padded, doc_padded = (
            with_halo(mixed_in, (("sp", 0),), 1),
            with_halo(doc_ids, (("sp", 0),), 1),
        )
        same_prev = (doc_padded[:-2] == doc_ids)[:, None]
        same_next = (doc_padded[2:] == doc_ids)[:, None]
        kernel_taps = taps[layer_index]
        convolved = (
            jnp.where(same_prev, kernel_taps[0] * padded[:-2].astype(jnp.float32), 0.0)
            + kernel_taps[1] * mixed_in.astype(jnp.float32)
            + jnp.where(same_next, kernel_taps[2] * padded[2:].astype(jnp.float32), 0.0)
        )
        gated = (gate_b.astype(jnp.float32) * convolved).astype(jnp.bfloat16)
        partials = jnp.dot(gated, gathered_out[layer_index], preferred_element_type=jnp.float32)
        summed = lax.psum_scatter(
            partials.astype(jnp.bfloat16), "tp", scatter_dimension=1, tiled=True
        ).astype(jnp.float32)
        current = (current.astype(jnp.float32) + summed).astype(jnp.bfloat16)
    return current


MESH = pl.DeviceIdType.MESH


def fused_kernel(S, T, L, stream_ref, docs_ref, gain_ref, gate_ref, input_ref, value_ref, taps_ref, outw_ref,
                 result_ref, win, wout, stage_in, stage_out, xfull, normed, cbuf, mpad, edge, halo, docall, docpad,
                 mprev, mnext, gated, dsrc, drcv, xsrc, xrcv, zsrc, zrcv, acc, zqsrc, zqrcv, xqsrc, xqrcv, accq,
                 own_sem, w_send, y_send, w_recv, x_sem, agz_send, agx_send, agc_send, ag_recv,
                 d_send, d_recv, x_send, x_recv, z_send, z_recv, h_send, h_recv, doc_send, doc_recv, pace,
                 zq_send, zq_recv, xq_send, xq_recv):
    s = lax.axis_index("sp")
    t = lax.axis_index("tp")
    Z = S // 2
    z, y = s // 2, s % 2
    zh, zl = z // 2, z % 2
    x, c = t // 2, t % 2
    X = T // 2
    rows = stream_ref.shape[0]
    depth = gate_ref.shape[1]
    half = taps_ref.shape[2] // 2
    ow = outw_ref.shape[2]
    width = stream_ref.shape[1]
    per = width // ow
    units = 4 * L
    other_y = s + 1 - 2 * y
    sibling = t + 1 - 2 * c
    across = lax.rem(t + 2, T)
    mate = s + 2 - 4 * zl
    theirs = 1 - zl
    sources = (input_ref, value_ref, gate_ref)
    bf, f32 = jnp.bfloat16, jnp.float32
    pending = []

    barrier = pltpu.get_barrier_semaphore()

    def greet(sp_index, tp_index):
        pl.semaphore_signal(barrier, inc=1, device_id=(sp_index, tp_index), device_id_type=MESH)

    for k in range(1, S):
        greet(lax.rem(s + k, S), t)
    greet(s, sibling)
    greet(s, across)

    def remote(src, dst, send_sem, recv_sem, target):
        return pltpu.make_async_remote_copy(src_ref=src, dst_ref=dst, send_sem=send_sem, recv_sem=recv_sem,
                                            device_id=target, device_id_type=MESH)

    def go(copy_of, cond=None):
        if cond is None:
            copy_of().start()
        else:
            pl.when(cond)(lambda: copy_of().start())
        pending.append((copy_of, cond))

    def slot(u, shard):
        layer, part = u // 4, u % 4
        if part < 3:
            return win.at[layer * 3 + part, pl.ds(pl.multiple_of(shard * depth, depth), depth)]
        return wout.at[layer, shard]

    def stage(u):
        layer, part = u // 4, u % 4
        return stage_in.at[layer * 3 + part] if part < 3 else stage_out.at[layer]

    def own_copy(u, which):
        layer, part = u // 4, u % 4
        pick = pl.ds(pl.multiple_of((zl if which == 0 else theirs) * half, half), half)
        source = outw_ref.at[layer, pick, :] if part == 3 else sources[part].at[layer, :, pick]
        return pltpu.make_async_copy(source, slot(u, s) if which == 0 else stage(u), own_sem.at[u, which])

    def piece(layer, plane, owner, i):
        return xfull.at[layer, plane, owner, i]

    def x_copy(i):
        return pltpu.make_async_copy(stream_ref.at[:, i * ow:(i + 1) * ow], piece(0, zl, t, i), x_sem.at[i])

    for i in range(per):
        x_copy(i).start()
    for u in range(units):
        for which in range(2):
            own_copy(u, which).start()

    pl.semaphore_wait(barrier, S + 1)

    def z_copy(u, k):
        plane = lax.rem(z + k, Z)
        return remote(slot(u, s) if k % 2 == 0 else stage(u), slot(u, s), w_send.at[u, k], w_recv.at[u, s],
                      (2 * plane + y, t))

    def y_copy(u, plane):
        shard = 2 * plane + y
        return remote(slot(u, shard), slot(u, shard), y_send.at[u, plane], w_recv.at[u, shard], (other_y, t))

    def own_y(u):
        go(lambda: y_copy(u, z))

    def begin(u):
        for k in range(1, Z):
            go(lambda k=k: z_copy(u, k))

    def arrived(u, shard):
        remote(slot(u, shard), slot(u, shard), y_send.at[u, z], w_recv.at[u, shard], (other_y, t)).wait_recv()

    def pump(u, low=1, high=Z):
        for k in range(low, high):
            plane = lax.rem(z + Z + (2 * zl - 1) * k, Z)
            arrived(u, 2 * plane + y)
            go(lambda plane=plane: y_copy(u, plane))

    def meet(u):
        pl.semaphore_signal(pace.at[u], inc=1, device_id=(s, sibling), device_id_type=MESH)
        pl.semaphore_wait(pace.at[u], 1)

    def need(u):
        for k in range(Z):
            plane = lax.rem(z + k, Z)
            arrived(u, 2 * plane + 1 - y)

    def agz(layer, i):
        return remote(piece(layer, zl, t, i), piece(layer, zl, t, i), agz_send.at[layer, i],
                      ag_recv.at[layer, zl, t, i], (mate, t))

    def agx(layer, plane, i):
        return remote(piece(layer, plane, t, i), piece(layer, plane, t, i), agx_send.at[layer, plane, i],
                      ag_recv.at[layer, plane, t, i], (s, across))

    def agc(layer, plane, owner, i):
        return remote(piece(layer, plane, owner, i), piece(layer, plane, owner, i),
                      agc_send.at[layer, plane, owner, i], ag_recv.at[layer, plane, owner, i], (s, sibling))

    def ag_wait(layer, plane, owner, i):
        remote(piece(layer, plane, owner, i), piece(layer, plane, owner, i), agz_send.at[layer, i],
               ag_recv.at[layer, plane, owner, i], (mate, t)).wait_recv()

    def ag_own(layer, i):
        go(lambda: agz(layer, i))
        go(lambda: agx(layer, zl, i))
        go(lambda: agc(layer, zl, t, i))

    def ag_from_z(layer, i):
        ag_wait(layer, theirs, t, i)
        go(lambda: agx(layer, theirs, i))
        go(lambda: agc(layer, theirs, t, i))

    def ag_from_x(layer, plane, i):
        ag_wait(layer, plane, across, i)
        go(lambda: agc(layer, plane, across, i))

    def ag_from_core(layer, plane):
        for i in range(per):
            ag_wait(layer, plane, sibling, i)
            ag_wait(layer, plane, lax.rem(sibling + 2, T), i)

    def doc_copy(k):
        return remote(docs_ref, docall.at[s], doc_send.at[k], doc_recv.at[s], (lax.rem(s + k, S), t))

    def group_block(b):
        return 2 * (2 * zh + b) + y

    def halo_copy(layer, b, side):
        target = lax.rem(group_block(b) + (1 if side == 0 else S - 1), S)
        core = 2 * (2 * (target // 4) + zl) + target % 2
        return remote(edge.at[layer, b, 1 - side], halo.at[layer, (target // 2) % 2, side],
                      h_send.at[layer, b, side], h_recv.at[layer, (target // 2) % 2, side], (core, t))

    def halo_wait(layer, b, side):
        remote(edge.at[layer, b, side], halo.at[layer, b, side], h_send.at[layer, b, side],
               h_recv.at[layer, b, side], (other_y, t)).wait_recv()

    for k in range(1, S):
        go(lambda k=k: doc_copy(k))
    for i in range(per):
        x_copy(i).wait()
        ag_own(0, i)
    for u in range(units):
        for which in range(2):
            own_copy(u, which).wait()
    for u in range(4):
        own_y(u)
    begin(0)
    begin(1)

    small = rows // 8

    def norm(layer, plane):
        def step(r, carry):
            at = pl.ds(pl.multiple_of(r * small, small), small)
            total = jnp.zeros((small, 1), f32)
            for q in range(T):
                for i in range(per):
                    wide = xfull[layer, plane, q, i, at, :].astype(f32)
                    total = total + jnp.sum(wide * wide, axis=-1, keepdims=True)
            scale = lax.rsqrt(total / (width * T) + epsilon)
            for q in range(T):
                for i in range(per):
                    wide = xfull[layer, plane, q, i, at, :].astype(f32)
                    low = q * width + i * ow
                    gain = gain_ref[layer:layer + 1, low:low + ow]
                    normed[plane, at, low:low + ow] = (wide * scale * gain).astype(bf)
            return carry

        lax.fori_loop(0, rows // small, step, 0)

    def project(layer, part, plane):
        product = jnp.dot(normed[plane], win[layer * 3 + part], preferred_element_type=f32).astype(bf)
        if part == 1:
            mixed = (cbuf[plane].astype(f32) * product.astype(f32)).astype(bf)
            mpad[plane, 8:8 + rows, :] = mixed.astype(f32)
        else:
            cbuf[plane] = product

    def columns(block, row):
        line = docall[block, row:row + 1, :].astype(f32)
        return jnp.transpose(jnp.broadcast_to(line, (128, 128)))

    def masks():
        docall[s] = docs_ref[...]
        for k in range(1, S):
            remote(docs_ref, docall.at[lax.rem(s + k, S)], doc_send.at[k], doc_recv.at[lax.rem(s + k, S)],
                   (other_y, t)).wait_recv()
        lines = rows // 128
        for b in range(2):
            block = group_block(b)
            for j in range(lines):
                docpad[8 + 128 * j:136 + 128 * j, :] = columns(block, j)
            before = columns(lax.rem(block + S - 1, S), lines - 1)[120:128, :]
            after = columns(lax.rem(block + 1, S), 0)[0:8, :]
            docpad[0:8, :] = jnp.where(block > 0, before, -1.0)
            docpad[8 + rows:16 + rows, :] = jnp.where(block < S - 1, after, -1.0)
            here = docpad[8:8 + rows, :]
            mprev[b] = jnp.where(docpad[7:7 + rows, :] == here, 1.0, 0.0)
            mnext[b] = jnp.where(docpad[9:9 + rows, :] == here, 1.0, 0.0)

    def send_edges(layer, b):
        edge[layer, b, 0] = mpad[b, 8:24, :].astype(bf)
        edge[layer, b, 1] = mpad[b, rows - 8:rows + 8, :].astype(bf)
        block = group_block(b)
        go(lambda: halo_copy(layer, b, 0), block < S - 1)
        go(lambda: halo_copy(layer, b, 1), block > 0)

    def convolve(layer):
        for b in range(2):
            block = group_block(b)
            empty = jnp.zeros((1, half), f32)

            @pl.when(block > 0)
            def _():
                halo_wait(layer, b, 0)
                mpad[b, 7:8, :] = halo[layer, b, 0, 15:16, :].astype(f32)

            @pl.when(block == 0)
            def _():
                mpad[b, 7:8, :] = empty

            @pl.when(block < S - 1)
            def _():
                halo_wait(layer, b, 1)
                mpad[b, 8 + rows:9 + rows, :] = halo[layer, b, 1, 0:1, :].astype(f32)

            @pl.when(block == S - 1)
            def _():
                mpad[b, 8 + rows:9 + rows, :] = empty

            for low in range(0, half, 128):
                lanes = slice(low, low + 128)
                tap = [jnp.where(zl == 0, taps_ref[j, layer:layer + 1, low:low + 128],
                                 taps_ref[j, layer:layer + 1, half + low:half + low + 128]) for j in range(3)]
                for r in range(0, rows, small):
                    before = tap[0] * mpad[b, r + 7:r + 7 + small, lanes]
                    middle = tap[1] * mpad[b, r + 8:r + 8 + small, lanes]
                    after = tap[2] * mpad[b, r + 9:r + 9 + small, lanes]
                    here = slice(r, r + small)
                    total = (jnp.where(mprev[b, here, :] > 0.5, before, 0.0) + middle
                             + jnp.where(mnext[b, here, :] > 0.5, after, 0.0))
                    gated[b, here, lanes] = (cbuf[b, here, lanes].astype(f32) * total).astype(bf)

    def owner_of(dx, dc):
        return lax.rem(x + dx, X) * 2 + lax.rem(c + dc, 2)

    def d_copy(layer, dx, i, tb):
        return remote(dsrc.at[layer, dx, i, tb], drcv.at[layer, dx, i, tb], d_send.at[layer, dx, i, tb],
                      d_recv.at[layer, dx, i, tb], (s, sibling))

    def xs_copy(layer, i, tb):
        return remote(xsrc.at[layer, i, tb], xrcv.at[layer, i, tb], x_send.at[layer, i, tb],
                      x_recv.at[layer, i, tb], (s, across))

    def zs_copy(layer, i):
        return remote(zsrc.at[layer, i], zrcv.at[layer, i], z_send.at[layer, i], z_recv.at[layer, i], (mate, t))

    first, second = y, 1 - y

    def partial(layer, dx, dc, i, tb):
        shard = owner_of(dx, dc) * per + i
        return jnp.dot(gated[lax.rem(theirs + tb, 2)], wout[layer, shard], preferred_element_type=f32)

    def each_block(use):
        def step(tb, carry):
            use(tb)
            return carry

        lax.fori_loop(0, 2, step, 0)

    def joined(layer, dx, i, tb):
        part = partial(layer, dx, 0, i, tb)
        d_copy(layer, dx, i, tb).wait_recv()
        return part + drcv[layer, dx, i, tb].astype(f32)

    def hand_over(layer, dx, i):
        def use(tb):
            dsrc[layer, dx, i, tb] = partial(layer, dx, 1, i, tb).astype(bf)
            d_copy(layer, dx, i, tb).start()

        each_block(use)

    def send_across(layer, i, tb):
        xsrc[layer, i, tb] = joined(layer, 1, i, tb).astype(bf)
        xs_copy(layer, i, tb).start()

    def hold(layer, i):
        def use(tb):
            acc[i, tb] = joined(layer, 0, i, tb)

        each_block(use)

    def to_mate(layer, i):
        xs_copy(layer, i, 0).wait_recv()
        zsrc[layer, i] = (acc[i, 0] + xrcv[layer, i, 0].astype(f32)).astype(bf)
        go(lambda: zs_copy(layer, i))

    def settle(layer, i, total):
        fresh = (xfull[layer, zl, t, i].astype(f32) + total).astype(bf)
        if layer + 1 < L:
            xfull[layer + 1, zl, t, i] = fresh
        else:
            for which in range(per):
                @pl.when(i == which)
                def _():
                    result_ref[:, which * ow:(which + 1) * ow] = fresh

    def finish(layer, i):
        xs_copy(layer, i, 1).wait_recv()
        zs_copy(layer, i).wait_recv()
        settle(layer, i, acc[i, 1] + xrcv[layer, i, 1].astype(f32) + zrcv[layer, i].astype(f32))

    def zq_copy(dx):
        return remote(zqsrc.at[dx], zqrcv.at[dx], zq_send.at[dx], zq_recv.at[dx], (mate, t))

    def xq_copy():
        return remote(xqsrc, xqrcv, xq_send, xq_recv, (s, across))

    def cross_first(layer, i, dx):
        zqsrc[dx] = joined(layer, dx, i, 0).astype(bf)
        go(lambda: zq_copy(dx))

    def cross_hold(layer, i, dx):
        held = joined(layer, dx, i, 1)
        if dx == 1:
            accq[...] = held
        else:
            acc[i, 1] = held

    def cross_sum():
        zq_copy(1).wait_recv()
        xqsrc[...] = (accq[...] + zqrcv[1].astype(f32)).astype(bf)
        go(xq_copy)

    def finish_crossed(layer, i):
        zq_copy(0).wait_recv()
        xq_copy().wait_recv()
        settle(layer, i, acc[i, 1] + zqrcv[0].astype(f32) + xqrcv[...].astype(f32))

    for layer in range(L):
        base = 4 * layer
        last = layer == L - 1
        if layer == 0:
            pump(0, 1, Z - 1)
            meet(0)
            begin(2)
            for i in range(per):
                ag_from_x(layer, zl, i)
            for i in range(per):
                ag_from_z(layer, i)
            pump(0, Z - 1, Z)
            masks()
            pump(1)
            meet(1)
            begin(3)
        else:
            pump(base + 2)
            ag_from_z(layer, first)
            ag_from_x(layer, zl, first)
            ag_from_x(layer, zl, second)
        ag_from_core(layer, zl)
        norm(layer, zl)
        if layer > 0:
            ag_from_z(layer, second)
        need(base)
        project(layer, 0, zl)
        if layer == 0:
            pump(2, 1, Z - 1)
        need(base + 1)
        project(layer, 1, zl)
        send_edges(layer, zl)
        if layer == 0:
            pump(2, Z - 1, Z)
        else:
            pump(base + 3)
        ag_from_x(layer, theirs, first)
        ag_from_x(layer, theirs, second)
        ag_from_core(layer, theirs)
        norm(layer, theirs)
        project(layer, 0, theirs)
        if layer == 0:
            pump(3, 1, 2)
        project(layer, 1, theirs)
        send_edges(layer, theirs)
        if layer == 0:
            pump(3, 2, Z)
        if not last:
            begin(base + 4)
        need(base + 2)
        project(layer, 2, zl)
        project(layer, 2, theirs)
        if not last:
            meet(base + 3)
            begin(base + 5)
        convolve(layer)
        if last:
            need(base + 3)
            hand_over(layer, 1, second)
            hand_over(layer, 1, first)
            cross_first(layer, second, 1)
            send_across(layer, first, 0)
            send_across(layer, first, 1)
            cross_hold(layer, second, 1)
            hand_over(layer, 0, second)
            hand_over(layer, 0, first)
            cross_first(layer, second, 0)
            hold(layer, first)
            cross_hold(layer, second, 0)
            to_mate(layer, first)
            cross_sum()
            finish(layer, first)
            finish_crossed(layer, second)
        else:
            hand_over(layer, 1, first)
            send_across(layer, first, 0)
            hand_over(layer, 0, first)
            hold(layer, first)
            need(base + 3)
            begin(base + 6)
            hand_over(layer, 1, second)
            send_across(layer, second, 0)
            send_across(layer, first, 1)
            send_across(layer, second, 1)
            for u in range(base + 4, base + 8):
                own_y(u)
            hand_over(layer, 0, second)
            hold(layer, second)
            to_mate(layer, first)
            to_mate(layer, second)
            pump(base + 4)
            finish(layer, first)
            ag_own(layer + 1, first)
            pump(base + 5)
            finish(layer, second)
            ag_own(layer + 1, second)
            begin(base + 7)

    for copy_of, cond in pending:
        if cond is None:
            copy_of().wait_send()
        else:
            pl.when(cond)(lambda copy_of=copy_of: copy_of().wait_send())
    for layer in range(L):
        for i in range(per):
            def drain(tb):
                for dx in range(2):
                    d_copy(layer, dx, i, tb).wait_send()

                @pl.when(jnp.logical_or(layer + 1 < L, i == first))
                def _():
                    xs_copy(layer, i, tb).wait_send()

            each_block(drain)


def fused(S, T, stream, doc_ids, norm_gain, gate_proj, input_gate, value_proj, taps, out_proj):
    rows, width = stream.shape
    L, depth, cols = gate_proj.shape
    ow = out_proj.shape[2]
    per, half = width // ow, cols // 2
    bf, f32, i32 = jnp.bfloat16, jnp.float32, jnp.int32
    docs = doc_ids.reshape(rows // 128, 128)
    vmem, hbm = pl.BlockSpec(memory_space=pltpu.VMEM), pl.BlockSpec(memory_space=pl.ANY)
    dma = pltpu.SemaphoreType.DMA
    scratch = [
        pltpu.VMEM((3 * L, S * depth, half), bf),
        pltpu.VMEM((L, S, half, ow), bf),
        pltpu.VMEM((3 * L, depth, half), bf),
        pltpu.VMEM((L, half, ow), bf),
        pltpu.VMEM((L, 2, T, per, rows, ow), bf),
        pltpu.VMEM((2, rows, T * width), bf),
        pltpu.VMEM((2, rows, half), bf),
        pltpu.VMEM((2, rows + 16, half), f32),
        pltpu.VMEM((L, 2, 2, 16, half), bf),
        pltpu.VMEM((L, 2, 2, 16, half), bf),
        pltpu.VMEM((S, rows // 128, 128), i32),
        pltpu.VMEM((rows + 16, 128), f32),
        pltpu.VMEM((2, rows, 128), f32),
        pltpu.VMEM((2, rows, 128), f32),
        pltpu.VMEM((2, rows, half), bf),
        pltpu.VMEM((L, 2, per, 2, rows, ow), bf),
        pltpu.VMEM((L, 2, per, 2, rows, ow), bf),
        pltpu.VMEM((L, per, 2, rows, ow), bf),
        pltpu.VMEM((L, per, 2, rows, ow), bf),
        pltpu.VMEM((L, per, rows, ow), bf),
        pltpu.VMEM((L, per, rows, ow), bf),
        pltpu.VMEM((per, 2, rows, ow), f32),
        pltpu.VMEM((2, rows, ow), bf),
        pltpu.VMEM((2, rows, ow), bf),
        pltpu.VMEM((rows, ow), bf),
        pltpu.VMEM((rows, ow), bf),
        pltpu.VMEM((rows, ow), f32),
        dma((4 * L, 2)),
        dma((4 * L, S // 2)),
        dma((4 * L, S // 2)),
        dma((4 * L, S)),
        dma((per,)),
        dma((L, per)),
        dma((L, 2, per)),
        dma((L, 2, T, per)),
        dma((L, 2, T, per)),
        dma((L, 2, per, 2)),
        dma((L, 2, per, 2)),
        dma((L, per, 2)),
        dma((L, per, 2)),
        dma((L, per)),
        dma((L, per)),
        dma((L, 2, 2)),
        dma((L, 2, 2)),
        dma((S,)),
        dma((S,)),
        pltpu.SemaphoreType.REGULAR((4 * L,)),
        dma((2,)),
        dma((2,)),
        dma,
        dma,
    ]
    return pl.pallas_call(
        functools.partial(fused_kernel, S, T, L),
        out_shape=jax.ShapeDtypeStruct((rows, width), bf),
        in_specs=[hbm, vmem, vmem, hbm, hbm, hbm, vmem, hbm],
        out_specs=vmem,
        scratch_shapes=scratch,
        compiler_params=pltpu.CompilerParams(
            collective_id=0, has_side_effects=True, vmem_limit_bytes=60 * 1024 * 1024),
    )(stream, docs, norm_gain, gate_proj, input_gate, value_proj, jnp.transpose(taps, (1, 0, 2)), out_proj)


def solution(mesh):
    sp, tp = mesh.shape["sp"], mesh.shape["tp"]

    def body(*arrays):
        (rows, width), cols, out_width = arrays[0].shape, arrays[3].shape[2], arrays[7].shape[2]
        aligned = out_width % 128 == 0 and cols % 256 == 0 and rows % 128 == 0 and width == 2 * out_width
        if aligned and sp % 4 == 0 and tp == 4:
            return fused(sp, tp, *arrays)
        return per_device(*arrays)

    in_specs = (
        P("sp", "tp"),
        P("sp"),
        P(),
        P(None, "sp", "tp"),
        P(None, "sp", "tp"),
        P(None, "sp", "tp"),
        P(None, None, "tp"),
        P(None, "tp", "sp"),
    )
    out_specs = P("sp", "tp")
    return jax.shard_map(
        body, mesh=mesh, in_specs=in_specs, out_specs=out_specs, check_vma=False
    )
```

```python
import functools

import jax
import jax.numpy as jnp
from jax import lax
from jax.experimental import pallas as pl
from jax.experimental.pallas import tpu as pltpu
from jax.sharding import PartitionSpec as P

epsilon = 1e-06


def with_halo(value, sides, width):
    for axis, dim in sides:
        size, length = (lax.axis_size(axis), value.shape[dim])
        up = [(i, (i + 1) % size) for i in range(size - 1)]
        down = [(j, i) for i, j in up]
        last = lax.slice_in_dim(value, length - width, length, axis=dim)
        leading = lax.slice_in_dim(value, 0, width, axis=dim)
        before = lax.ppermute(last, axis, up)
        after = lax.ppermute(leading, axis, down)
        value = jnp.concatenate([before, value, after], axis=dim)
    return value


def per_device(stream, doc_ids, norm_gain, gate_proj, input_gate, value_proj, taps, out_proj):
    layers = gate_proj.shape[0]
    gathered_in = (
        lax.all_gather(gate_proj, "sp", axis=1, tiled=True),
        lax.all_gather(input_gate, "sp", axis=1, tiled=True),
        lax.all_gather(value_proj, "sp", axis=1, tiled=True),
    )
    gathered_out = lax.all_gather(out_proj, "sp", axis=2, tiled=True)
    current = stream
    for layer_index in range(layers):
        full_rows = lax.all_gather(current, "tp", axis=1, tiled=True)
        widened = full_rows.astype(jnp.float32)
        scale = lax.rsqrt(jnp.mean(widened * widened, axis=-1, keepdims=True) + epsilon)
        normed = (widened * scale * norm_gain[layer_index]).astype(jnp.bfloat16)
        gate_b = jnp.dot(normed, gathered_in[0][layer_index], preferred_element_type=jnp.float32)
        gate_c = jnp.dot(normed, gathered_in[1][layer_index], preferred_element_type=jnp.float32)
        values = jnp.dot(normed, gathered_in[2][layer_index], preferred_element_type=jnp.float32)
        gate_b = gate_b.astype(jnp.bfloat16)
        gate_c = gate_c.astype(jnp.bfloat16)
        values = values.astype(jnp.bfloat16)
        mixed_in = (gate_c.astype(jnp.float32) * values.astype(jnp.float32)).astype(jnp.bfloat16)
        padded, doc_padded = (
            with_halo(mixed_in, (("sp", 0),), 1),
            with_halo(doc_ids, (("sp", 0),), 1),
        )
        same_prev = (doc_padded[:-2] == doc_ids)[:, None]
        same_next = (doc_padded[2:] == doc_ids)[:, None]
        kernel_taps = taps[layer_index]
        convolved = (
            jnp.where(same_prev, kernel_taps[0] * padded[:-2].astype(jnp.float32), 0.0)
            + kernel_taps[1] * mixed_in.astype(jnp.float32)
            + jnp.where(same_next, kernel_taps[2] * padded[2:].astype(jnp.float32), 0.0)
        )
        gated = (gate_b.astype(jnp.float32) * convolved).astype(jnp.bfloat16)
        partials = jnp.dot(gated, gathered_out[layer_index], preferred_element_type=jnp.float32)
        summed = lax.psum_scatter(
            partials.astype(jnp.bfloat16), "tp", scatter_dimension=1, tiled=True
        ).astype(jnp.float32)
        current = (current.astype(jnp.float32) + summed).astype(jnp.bfloat16)
    return current


MESH = pl.DeviceIdType.MESH


def fused_kernel(S, T, L, stream_ref, docs_ref, gain_ref, gate_ref, input_ref, value_ref, taps_ref, outw_ref,
                 result_ref, win, wout, stage_in, stage_out, xfull, normed, cbuf, mpad, edge, halo, docall, docpad,
                 mprev, mnext, gated, dsrc, drcv, xsrc, xrcv, zsrc, zrcv, acc, zqsrc, zqrcv, xqsrc, xqrcv, accq,
                 own_sem, w_send, y_send, w_recv, x_sem, agz_send, agx_send, agc_send, ag_recv,
                 d_send, d_recv, x_send, x_recv, z_send, z_recv, h_send, h_recv, doc_send, doc_recv, pace,
                 zq_send, zq_recv, xq_send, xq_recv):
    s = lax.axis_index("sp")
    t = lax.axis_index("tp")
    Z = S // 2
    z, y = s // 2, s % 2
    zh, zl = z // 2, z % 2
    x, c = t // 2, t % 2
    X = T // 2
    rows = stream_ref.shape[0]
    depth = gate_ref.shape[1]
    half = taps_ref.shape[2] // 2
    ow = outw_ref.shape[2]
    width = stream_ref.shape[1]
    per = width // ow
    units = 4 * L
    other_y = s + 1 - 2 * y
    sibling = t + 1 - 2 * c
    across = lax.rem(t + 2, T)
    mate = s + 2 - 4 * zl
    theirs = 1 - zl
    sources = (input_ref, value_ref, gate_ref)
    bf, f32 = jnp.bfloat16, jnp.float32
    pending = []

    barrier = pltpu.get_barrier_semaphore()

    def greet(sp_index, tp_index):
        pl.semaphore_signal(barrier, inc=1, device_id=(sp_index, tp_index), device_id_type=MESH)

    for k in range(1, S):
        greet(lax.rem(s + k, S), t)
    greet(s, sibling)
    greet(s, across)

    def remote(src, dst, send_sem, recv_sem, target):
        return pltpu.make_async_remote_copy(src_ref=src, dst_ref=dst, send_sem=send_sem, recv_sem=recv_sem,
                                            device_id=target, device_id_type=MESH)

    def go(copy_of, cond=None):
        if cond is None:
            copy_of().start()
        else:
            pl.when(cond)(lambda: copy_of().start())
        pending.append((copy_of, cond))

    def slot(u, shard):
        layer, part = u // 4, u % 4
        if part < 3:
            return win.at[layer * 3 + part, pl.ds(pl.multiple_of(shard * depth, depth), depth)]
        return wout.at[layer, shard]

    def stage(u):
        layer, part = u // 4, u % 4
        return stage_in.at[layer * 3 + part] if part < 3 else stage_out.at[layer]

    def own_copy(u, which):
        layer, part = u // 4, u % 4
        pick = pl.ds(pl.multiple_of((zl if which == 0 else theirs) * half, half), half)
        source = outw_ref.at[layer, pick, :] if part == 3 else sources[part].at[layer, :, pick]
        return pltpu.make_async_copy(source, slot(u, s) if which == 0 else stage(u), own_sem.at[u, which])

    def piece(layer, plane, owner, i):
        return xfull.at[layer, plane, owner, i]

    def x_copy(i):
        return pltpu.make_async_copy(stream_ref.at[:, i * ow:(i + 1) * ow], piece(0, zl, t, i), x_sem.at[i])

    for i in range(per):
        x_copy(i).start()
    for u in range(units):
        for which in range(2):
            own_copy(u, which).start()

    pl.semaphore_wait(barrier, S + 1)

    def z_copy(u, k):
        plane = lax.rem(z + k, Z)
        return remote(slot(u, s) if k % 2 == 0 else stage(u), slot(u, s), w_send.at[u, k], w_recv.at[u, s],
                      (2 * plane + y, t))

    def y_copy(u, plane):
        shard = 2 * plane + y
        return remote(slot(u, shard), slot(u, shard), y_send.at[u, plane], w_recv.at[u, shard], (other_y, t))

    def own_y(u):
        go(lambda: y_copy(u, z))

    def begin(u):
        for k in range(1, Z):
            go(lambda k=k: z_copy(u, k))

    def arrived(u, shard):
        remote(slot(u, shard), slot(u, shard), y_send.at[u, z], w_recv.at[u, shard], (other_y, t)).wait_recv()

    def pump(u, low=1, high=Z):
        for k in range(low, high):
            plane = lax.rem(z + Z + (2 * zl - 1) * k, Z)
            arrived(u, 2 * plane + y)
            go(lambda plane=plane: y_copy(u, plane))

    def meet(u):
        pl.semaphore_signal(pace.at[u], inc=1, device_id=(s, sibling), device_id_type=MESH)
        pl.semaphore_wait(pace.at[u], 1)

    def need(u):
        for k in range(Z):
            plane = lax.rem(z + k, Z)
            arrived(u, 2 * plane + 1 - y)

    def agz(layer, i):
        return remote(piece(layer, zl, t, i), piece(layer, zl, t, i), agz_send.at[layer, i],
                      ag_recv.at[layer, zl, t, i], (mate, t))

    def agx(layer, plane, i):
        return remote(piece(layer, plane, t, i), piece(layer, plane, t, i), agx_send.at[layer, plane, i],
                      ag_recv.at[layer, plane, t, i], (s, across))

    def agc(layer, plane, owner, i):
        return remote(piece(layer, plane, owner, i), piece(layer, plane, owner, i),
                      agc_send.at[layer, plane, owner, i], ag_recv.at[layer, plane, owner, i], (s, sibling))

    def ag_wait(layer, plane, owner, i):
        remote(piece(layer, plane, owner, i), piece(layer, plane, owner, i), agz_send.at[layer, i],
               ag_recv.at[layer, plane, owner, i], (mate, t)).wait_recv()

    def ag_own(layer, i):
        go(lambda: agz(layer, i))
        go(lambda: agx(layer, zl, i))
        go(lambda: agc(layer, zl, t, i))

    def ag_from_z(layer, i):
        ag_wait(layer, theirs, t, i)
        go(lambda: agx(layer, theirs, i))
        go(lambda: agc(layer, theirs, t, i))

    def ag_from_x(layer, plane, i):
        ag_wait(layer, plane, across, i)
        go(lambda: agc(layer, plane, across, i))

    def ag_from_core(layer, plane):
        for i in range(per):
            ag_wait(layer, plane, sibling, i)
            ag_wait(layer, plane, lax.rem(sibling + 2, T), i)

    def doc_copy(k):
        return remote(docs_ref, docall.at[s], doc_send.at[k], doc_recv.at[s], (lax.rem(s + k, S), t))

    def group_block(b):
        return 2 * (2 * zh + b) + y

    def halo_copy(layer, b, side):
        target = lax.rem(group_block(b) + (1 if side == 0 else S - 1), S)
        core = 2 * (2 * (target // 4) + zl) + target % 2
        return remote(edge.at[layer, b, 1 - side], halo.at[layer, (target // 2) % 2, side],
                      h_send.at[layer, b, side], h_recv.at[layer, (target // 2) % 2, side], (core, t))

    def halo_wait(layer, b, side):
        remote(edge.at[layer, b, side], halo.at[layer, b, side], h_send.at[layer, b, side],
               h_recv.at[layer, b, side], (other_y, t)).wait_recv()

    for k in range(1, S):
        go(lambda k=k: doc_copy(k))
    for i in range(per):
        x_copy(i).wait()
        ag_own(0, i)
    for u in range(units):
        for which in range(2):
            own_copy(u, which).wait()
    for u in range(4):
        own_y(u)
    begin(0)
    begin(1)

    small = rows // 8

    def norm(layer, plane):
        def step(r, carry):
            at = pl.ds(pl.multiple_of(r * small, small), small)
            total = jnp.zeros((small, 1), f32)
            for q in range(T):
                for i in range(per):
                    wide = xfull[layer, plane, q, i, at, :].astype(f32)
                    total = total + jnp.sum(wide * wide, axis=-1, keepdims=True)
            scale = lax.rsqrt(total / (width * T) + epsilon)
            for q in range(T):
                for i in range(per):
                    wide = xfull[layer, plane, q, i, at, :].astype(f32)
                    low = q * width + i * ow
                    gain = gain_ref[layer:layer + 1, low:low + ow]
                    normed[plane, at, low:low + ow] = (wide * scale * gain).astype(bf)
            return carry

        lax.fori_loop(0, rows // small, step, 0)

    def project(layer, part, plane):
        product = jnp.dot(normed[plane], win[layer * 3 + part], preferred_element_type=f32).astype(bf)
        if part == 1:
            mixed = (cbuf[plane].astype(f32) * product.astype(f32)).astype(bf)
            mpad[plane, 8:8 + rows, :] = mixed.astype(f32)
        else:
            cbuf[plane] = product

    def columns(block, row):
        line = docall[block, row:row + 1, :].astype(f32)
        return jnp.transpose(jnp.broadcast_to(line, (128, 128)))

    def masks():
        docall[s] = docs_ref[...]
        for k in range(1, S):
            remote(docs_ref, docall.at[lax.rem(s + k, S)], doc_send.at[k], doc_recv.at[lax.rem(s + k, S)],
                   (other_y, t)).wait_recv()
        lines = rows // 128
        for b in range(2):
            block = group_block(b)
            for j in range(lines):
                docpad[8 + 128 * j:136 + 128 * j, :] = columns(block, j)
            before = columns(lax.rem(block + S - 1, S), lines - 1)[120:128, :]
            after = columns(lax.rem(block + 1, S), 0)[0:8, :]
            docpad[0:8, :] = jnp.where(block > 0, before, -1.0)
            docpad[8 + rows:16 + rows, :] = jnp.where(block < S - 1, after, -1.0)
            here = docpad[8:8 + rows, :]
            mprev[b] = jnp.where(docpad[7:7 + rows, :] == here, 1.0, 0.0)
            mnext[b] = jnp.where(docpad[9:9 + rows, :] == here, 1.0, 0.0)

    def send_edges(layer, b):
        edge[layer, b, 0] = mpad[b, 8:24, :].astype(bf)
        edge[layer, b, 1] = mpad[b, rows - 8:rows + 8, :].astype(bf)
        block = group_block(b)
        go(lambda: halo_copy(layer, b, 0), block < S - 1)
        go(lambda: halo_copy(layer, b, 1), block > 0)

    def convolve(layer):
        for b in range(2):
            block = group_block(b)
            empty = jnp.zeros((1, half), f32)

            @pl.when(block > 0)
            def _():
                halo_wait(layer, b, 0)
                mpad[b, 7:8, :] = halo[layer, b, 0, 15:16, :].astype(f32)

            @pl.when(block == 0)
            def _():
                mpad[b, 7:8, :] = empty

            @pl.when(block < S - 1)
            def _():
                halo_wait(layer, b, 1)
                mpad[b, 8 + rows:9 + rows, :] = halo[layer, b, 1, 0:1, :].astype(f32)

            @pl.when(block == S - 1)
            def _():
                mpad[b, 8 + rows:9 + rows, :] = empty

            for low in range(0, half, 128):
                lanes = slice(low, low + 128)
                tap = [jnp.where(zl == 0, taps_ref[j, layer:layer + 1, low:low + 128],
                                 taps_ref[j, layer:layer + 1, half + low:half + low + 128]) for j in range(3)]
                for r in range(0, rows, small):
                    before = tap[0] * mpad[b, r + 7:r + 7 + small, lanes]
                    middle = tap[1] * mpad[b, r + 8:r + 8 + small, lanes]
                    after = tap[2] * mpad[b, r + 9:r + 9 + small, lanes]
                    here = slice(r, r + small)
                    total = (jnp.where(mprev[b, here, :] > 0.5, before, 0.0) + middle
                             + jnp.where(mnext[b, here, :] > 0.5, after, 0.0))
                    gated[b, here, lanes] = (cbuf[b, here, lanes].astype(f32) * total).astype(bf)

    def owner_of(dx, dc):
        return lax.rem(x + dx, X) * 2 + lax.rem(c + dc, 2)

    def d_copy(layer, dx, i, tb):
        return remote(dsrc.at[layer, dx, i, tb], drcv.at[layer, dx, i, tb], d_send.at[layer, dx, i, tb],
                      d_recv.at[layer, dx, i, tb], (s, sibling))

    def xs_copy(layer, i, tb):
        return remote(xsrc.at[layer, i, tb], xrcv.at[layer, i, tb], x_send.at[layer, i, tb],
                      x_recv.at[layer, i, tb], (s, across))

    def zs_copy(layer, i):
        return remote(zsrc.at[layer, i], zrcv.at[layer, i], z_send.at[layer, i], z_recv.at[layer, i], (mate, t))

    first, second = y, 1 - y

    def partial(layer, dx, dc, i, tb):
        shard = owner_of(dx, dc) * per + i
        return jnp.dot(gated[lax.rem(theirs + tb, 2)], wout[layer, shard], preferred_element_type=f32)

    def each_block(use):
        def step(tb, carry):
            use(tb)
            return carry

        lax.fori_loop(0, 2, step, 0)

    def joined(layer, dx, i, tb):
        part = partial(layer, dx, 0, i, tb)
        d_copy(layer, dx, i, tb).wait_recv()
        return part + drcv[layer, dx, i, tb].astype(f32)

    def hand_over(layer, dx, i):
        def use(tb):
            dsrc[layer, dx, i, tb] = partial(layer, dx, 1, i, tb).astype(bf)
            d_copy(layer, dx, i, tb).start()

        each_block(use)

    def send_across(layer, i, tb):
        xsrc[layer, i, tb] = joined(layer, 1, i, tb).astype(bf)
        xs_copy(layer, i, tb).start()

    def hold(layer, i):
        def use(tb):
            acc[i, tb] = joined(layer, 0, i, tb)

        each_block(use)

    def to_mate(layer, i):
        xs_copy(layer, i, 0).wait_recv()
        zsrc[layer, i] = (acc[i, 0] + xrcv[layer, i, 0].astype(f32)).astype(bf)
        go(lambda: zs_copy(layer, i))

    def settle(layer, i, total):
        fresh = (xfull[layer, zl, t, i].astype(f32) + total).astype(bf)
        if layer + 1 < L:
            xfull[layer + 1, zl, t, i] = fresh
        else:
            for which in range(per):
                @pl.when(i == which)
                def _():
                    result_ref[:, which * ow:(which + 1) * ow] = fresh

    def finish(layer, i):
        xs_copy(layer, i, 1).wait_recv()
        zs_copy(layer, i).wait_recv()
        settle(layer, i, acc[i, 1] + xrcv[layer, i, 1].astype(f32) + zrcv[layer, i].astype(f32))

    def zq_copy(dx):
        return remote(zqsrc.at[dx], zqrcv.at[dx], zq_send.at[dx], zq_recv.at[dx], (mate, t))

    def xq_copy():
        return remote(xqsrc, xqrcv, xq_send, xq_recv, (s, across))

    def cross_first(layer, i, dx):
        zqsrc[dx] = joined(layer, dx, i, 0).astype(bf)
        go(lambda: zq_copy(dx))

    def cross_hold(layer, i, dx):
        held = joined(layer, dx, i, 1)
        if dx == 1:
            accq[...] = held
        else:
            acc[i, 1] = held

    def cross_sum():
        zq_copy(1).wait_recv()
        xqsrc[...] = (accq[...] + zqrcv[1].astype(f32)).astype(bf)
        go(xq_copy)

    def finish_crossed(layer, i):
        zq_copy(0).wait_recv()
        xq_copy().wait_recv()
        settle(layer, i, acc[i, 1] + zqrcv[0].astype(f32) + xqrcv[...].astype(f32))

    for layer in range(L):
        base = 4 * layer
        last = layer == L - 1
        if layer == 0:
            pump(0, 1, Z - 1)
            meet(0)
            begin(2)
            for i in range(per):
                ag_from_x(layer, zl, i)
            for i in range(per):
                ag_from_z(layer, i)
            pump(0, Z - 1, Z)
            masks()
            pump(1)
            meet(1)
            begin(3)
        else:
            pump(base + 2)
            ag_from_z(layer, first)
            ag_from_x(layer, zl, first)
            ag_from_x(layer, zl, second)
        ag_from_core(layer, zl)
        norm(layer, zl)
        if layer > 0:
            ag_from_z(layer, second)
        need(base)
        project(layer, 0, zl)
        if layer == 0:
            pump(2, 1, Z - 1)
        need(base + 1)
        project(layer, 1, zl)
        send_edges(layer, zl)
        if layer == 0:
            pump(2, Z - 1, Z)
        else:
            need(base + 2)
            project(layer, 2, zl)
            pump(base + 3)
        ag_from_x(layer, theirs, first)
        ag_from_x(layer, theirs, second)
        ag_from_core(layer, theirs)
        norm(layer, theirs)
        project(layer, 0, theirs)
        if layer == 0:
            pump(3, 1, 2)
        project(layer, 1, theirs)
        send_edges(layer, theirs)
        if layer == 0:
            pump(3, 2, Z)
        if not last:
            begin(base + 4)
        if layer == 0:
            need(base + 2)
            project(layer, 2, zl)
        project(layer, 2, theirs)
        if not last:
            meet(base + 3)
            begin(base + 5)
        convolve(layer)
        if last:
            need(base + 3)
            hand_over(layer, 1, second)
            hand_over(layer, 1, first)
            cross_first(layer, second, 1)
            send_across(layer, first, 0)
            send_across(layer, first, 1)
            cross_hold(layer, second, 1)
            hand_over(layer, 0, second)
            hand_over(layer, 0, first)
            cross_first(layer, second, 0)
            hold(layer, first)
            cross_hold(layer, second, 0)
            to_mate(layer, first)
            cross_sum()
            finish(layer, first)
            finish_crossed(layer, second)
        else:
            hand_over(layer, 1, first)
            send_across(layer, first, 0)
            hand_over(layer, 0, first)
            hold(layer, first)
            need(base + 3)
            begin(base + 6)
            hand_over(layer, 1, second)
            send_across(layer, second, 0)
            send_across(layer, first, 1)
            send_across(layer, second, 1)
            for u in range(base + 4, base + 8):
                own_y(u)
            hand_over(layer, 0, second)
            hold(layer, second)
            to_mate(layer, first)
            to_mate(layer, second)
            pump(base + 4)
            finish(layer, first)
            ag_own(layer + 1, first)
            pump(base + 5)
            finish(layer, second)
            ag_own(layer + 1, second)
            begin(base + 7)

    for copy_of, cond in pending:
        if cond is None:
            copy_of().wait_send()
        else:
            pl.when(cond)(lambda copy_of=copy_of: copy_of().wait_send())
    for layer in range(L):
        for i in range(per):
            def drain(tb):
                for dx in range(2):
                    d_copy(layer, dx, i, tb).wait_send()

                @pl.when(jnp.logical_or(layer + 1 < L, i == first))
                def _():
                    xs_copy(layer, i, tb).wait_send()

            each_block(drain)


def fused(S, T, stream, doc_ids, norm_gain, gate_proj, input_gate, value_proj, taps, out_proj):
    rows, width = stream.shape
    L, depth, cols = gate_proj.shape
    ow = out_proj.shape[2]
    per, half = width // ow, cols // 2
    bf, f32, i32 = jnp.bfloat16, jnp.float32, jnp.int32
    docs = doc_ids.reshape(rows // 128, 128)
    vmem, hbm = pl.BlockSpec(memory_space=pltpu.VMEM), pl.BlockSpec(memory_space=pl.ANY)
    dma = pltpu.SemaphoreType.DMA
    scratch = [
        pltpu.VMEM((3 * L, S * depth, half), bf),
        pltpu.VMEM((L, S, half, ow), bf),
        pltpu.VMEM((3 * L, depth, half), bf),
        pltpu.VMEM((L, half, ow), bf),
        pltpu.VMEM((L, 2, T, per, rows, ow), bf),
        pltpu.VMEM((2, rows, T * width), bf),
        pltpu.VMEM((2, rows, half), bf),
        pltpu.VMEM((2, rows + 16, half), f32),
        pltpu.VMEM((L, 2, 2, 16, half), bf),
        pltpu.VMEM((L, 2, 2, 16, half), bf),
        pltpu.VMEM((S, rows // 128, 128), i32),
        pltpu.VMEM((rows + 16, 128), f32),
        pltpu.VMEM((2, rows, 128), f32),
        pltpu.VMEM((2, rows, 128), f32),
        pltpu.VMEM((2, rows, half), bf),
        pltpu.VMEM((L, 2, per, 2, rows, ow), bf),
        pltpu.VMEM((L, 2, per, 2, rows, ow), bf),
        pltpu.VMEM((L, per, 2, rows, ow), bf),
        pltpu.VMEM((L, per, 2, rows, ow), bf),
        pltpu.VMEM((L, per, rows, ow), bf),
        pltpu.VMEM((L, per, rows, ow), bf),
        pltpu.VMEM((per, 2, rows, ow), f32),
        pltpu.VMEM((2, rows, ow), bf),
        pltpu.VMEM((2, rows, ow), bf),
        pltpu.VMEM((rows, ow), bf),
        pltpu.VMEM((rows, ow), bf),
        pltpu.VMEM((rows, ow), f32),
        dma((4 * L, 2)),
        dma((4 * L, S // 2)),
        dma((4 * L, S // 2)),
        dma((4 * L, S)),
        dma((per,)),
        dma((L, per)),
        dma((L, 2, per)),
        dma((L, 2, T, per)),
        dma((L, 2, T, per)),
        dma((L, 2, per, 2)),
        dma((L, 2, per, 2)),
        dma((L, per, 2)),
        dma((L, per, 2)),
        dma((L, per)),
        dma((L, per)),
        dma((L, 2, 2)),
        dma((L, 2, 2)),
        dma((S,)),
        dma((S,)),
        pltpu.SemaphoreType.REGULAR((4 * L,)),
        dma((2,)),
        dma((2,)),
        dma,
        dma,
    ]
    return pl.pallas_call(
        functools.partial(fused_kernel, S, T, L),
        out_shape=jax.ShapeDtypeStruct((rows, width), bf),
        in_specs=[hbm, vmem, vmem, hbm, hbm, hbm, vmem, hbm],
        out_specs=vmem,
        scratch_shapes=scratch,
        compiler_params=pltpu.CompilerParams(
            collective_id=0, has_side_effects=True, vmem_limit_bytes=60 * 1024 * 1024),
    )(stream, docs, norm_gain, gate_proj, input_gate, value_proj, jnp.transpose(taps, (1, 0, 2)), out_proj)


def solution(mesh):
    sp, tp = mesh.shape["sp"], mesh.shape["tp"]

    def body(*arrays):
        (rows, width), cols, out_width = arrays[0].shape, arrays[3].shape[2], arrays[7].shape[2]
        aligned = out_width % 128 == 0 and cols % 256 == 0 and rows % 128 == 0 and width == 2 * out_width
        if aligned and sp % 4 == 0 and tp == 4:
            return fused(sp, tp, *arrays)
        return per_device(*arrays)

    in_specs = (
        P("sp", "tp"),
        P("sp"),
        P(),
        P(None, "sp", "tp"),
        P(None, "sp", "tp"),
        P(None, "sp", "tp"),
        P(None, None, "tp"),
        P(None, "tp", "sp"),
    )
    out_specs = P("sp", "tp")
    return jax.shard_map(
        body, mesh=mesh, in_specs=in_specs, out_specs=out_specs, check_vma=False
    )
```
